512 devices in a mesh: sp: 32 (over z, core), tp: 16 (over y, x).
Axes of the slice: x: 4, y: 4, z: 16, core: 2. Of those that a mesh axis runs over, the one named last changes fastest.
Arguments:
- layer_input: bfloat16 [8192, 2048], P('sp', 'tp'), may hold values from -6 to 6
- doc_ids: int32 [8192], P('sp'), may hold values from 0 to 7, never falling along the last dimension, each value on 1 to 1536 neighbouring positions
- routes: int32 [8192, 2], P('sp'), may hold values from 0 to 31, all different within a row; in each aligned block of 256 rows (0 to 255, 256 to 511, ...) at most 22 rows name the same one
- route_weight: float32 [8192, 2], P('sp'), may hold values from 0.2 to 2
- pool_weight: bfloat16 [4, 512, 512], replicated, may hold values from -0.25 to 0.25
- pool_scale: float32 [2048], replicated, may hold values from 0.1 to 1.9
- norm1_gain: float32 [2048], replicated, may hold values from 0.3 to 3
- norm1_bias: float32 [2048], replicated, may hold values from -3 to 3
- expert_gate: bfloat16 [32, 2048, 2048], P('sp', None, 'tp'), may hold values from -0.125 to 0.125
- expert_up: bfloat16 [32, 2048, 2048], P('sp', None, 'tp'), may hold values from -0.125 to 0.125
- expert_down: bfloat16 [32, 2048, 2048], P('sp', 'tp'), may hold values from -0.125 to 0.125
- shared_gate: bfloat16 [2048, 1024], P(None, 'tp'), may hold values from -0.125 to 0.125
- shared_up: bfloat16 [2048, 1024], P(None, 'tp'), may hold values from -0.125 to 0.125
- shared_down: bfloat16 [1024, 2048], P('tp'), may hold values from -0.1875 to 0.1875
- norm2_gain: float32 [2048], P('tp'), may hold values from 0.1 to 1.9
- norm2_bias: float32 [2048], P('tp'), may hold values from -3 to 3
Outputs:
- settled: bfloat16 [8192, 2048], P('sp', 'tp')
The draws below stay inside these ranges and needn't reach their ends.
Inputs may be any that keep to these rules, and one draw needn't show every extreme that they name: `routes`: in each aligned block of 256 rows no expert is named by more than 22 picks, a bound that some block reaches. `doc_ids`: never falling along the positions; each document spans 1 to 1536 positions.
All inputs are finite; a program needn't handle non-finite values.
Results may differ from the reference program's by a relative error of at most 0.013.
Values may be sent and summed in bfloat16 or wider, within the bound.
No kernel may reach another device: no remote copies, remote signals or barrier semaphores. Data moves between devices by JAX's collectives and lax.ppermute only.
A program may use at most 64 MiB of HBM per device.

```python
import math
import jax
import jax.numpy as jnp
import numpy as np
from jax import lax

D = 2048
GROUPS = 4
GROUP_WIDTH = 512
EXPERT_WIDTH = 2048
SHARED_WIDTH = 1024
TOP_K = 2
TOK_DEV = 256
TOKENS = 8192
EXPERTS = 32
CAPACITY = 22
N_SP = 32
N_TP = 16


def levels(stream_key, dims, cuts, low, top_value):
    level = 1.0
    for axis_at, shards_of in cuts:
        steps = jax.random.uniform(jax.random.fold_in(jax.random.fold_in(stream_key, 6), axis_at), (shards_of,), jnp.float32, low / len(cuts), top_value / len(cuts))
        level = level * jnp.repeat(jnp.exp(steps), dims[axis_at] // shards_of).reshape((-1,) + (1,) * (len(dims) - 1 - axis_at))
    return level


def profile(amount, total, reach, slope):
    weights = [(1 << 20) // math.isqrt(standing ** slope) + 1 for standing in range(2, amount + 1)]
    rest, holding = total - reach - (amount - 1), [1] * (amount - 1)
    while rest > 0:
        movable = [i for i in range(amount - 1) if holding[i] < reach]
        mass, budget = sum([weights[i] for i in movable]), rest
        for i in movable:
            extra = min(reach - holding[i], max(1, budget * weights[i] // mass), rest)
            holding[i] = holding[i] + extra
            rest = rest - extra
    return np.array([reach] + holding)


def uneven_parts(own_key, number_of, total, most, slope):
    if number_of == 2:
        one = jax.random.randint(own_key, (), max(1, total - most), min(most, total - 1) + 1)
        return jnp.stack([one, total - one])
    sizes = jnp.asarray(profile(number_of, total, most, slope), jnp.int32)
    couples = (number_of - 1) // 2
    donor, sink = sizes[1:1 + 2 * couples:2], sizes[2:2 + 2 * couples:2]
    slack = jnp.minimum(donor - 1, most - sink)
    moved = jax.random.randint(jax.random.fold_in(own_key, 1), (couples,), 0, 1 << 20) % (slack + 1)
    sizes = sizes.at[1:1 + 2 * couples:2].set(donor - moved).at[2:2 + 2 * couples:2].set(sink + moved)
    return sizes[jax.random.permutation(jax.random.fold_in(own_key, 2), number_of)]


def routed_block(stream_key, own, number, rows, amount, top, bound, lean):
    sequence = jax.random.permutation(stream_key, amount)
    packed, common = load_shares(amount, rows * top, bound, lean, True), load_shares(amount, rows * top, bound, lean, False)
    places = jnp.arange(amount)

    def named(sizes, rotation):
        used = int((sizes > 0).sum())
        fixed = max(1, used // 4)
        moved = fixed + (places - fixed + rotation * (used - fixed)) % max(1, amount - fixed)
        return jnp.zeros((amount,), jnp.int32).at[sequence[jnp.where(places < fixed, places, moved)]].set(jnp.asarray(sizes, jnp.int32))

    sizes = jnp.where(number % 4 == 0, named(packed, number // 4), named(common, number - number // 4 - 1))
    mixed = jax.random.permutation(jax.random.fold_in(own, 3), amount)
    donor, taker = mixed[0:amount // 2 * 2:2], mixed[1:amount // 2 * 2:2]
    slack = jnp.minimum(sizes[donor] - 1, bound - sizes[taker]) // 2
    slack = jnp.where((donor == sequence[0]) | (taker == sequence[0]) | (sizes[taker] == 0), 0, jnp.maximum(slack, 0))
    moved = jax.random.randint(jax.random.fold_in(own, 4), (amount // 2,), 0, 1 << 20) % (slack + 1)
    sizes = sizes.at[donor].add(-moved).at[taker].add(moved)
    items = jnp.searchsorted(jnp.cumsum(sizes), jnp.arange(rows * top), side="right").astype(jnp.int32)
    listing = items.reshape(top, rows).T
    listing = listing[jax.random.permutation(jax.random.fold_in(own, 1), rows)]
    rotation = jax.random.randint(jax.random.fold_in(own, 2), (rows, 1), 0, top)
    return jnp.take_along_axis(listing, (jnp.arange(top)[None, :] + rotation) % top, axis=1)


def load_shares(number_of, total, reach, slope, full):
    portions = [(1 << 20) // math.isqrt(grade ** slope) + 1 for grade in range(1, number_of + 1)]
    largest = reach if full else min(reach, max(-(-total // number_of), total * portions[0] // sum(portions)))
    least = 1 if total - largest >= number_of - 1 else 0
    holding, spare = [largest] + [least] * (number_of - 1), total - largest - least * (number_of - 1)
    while spare > 0:
        movable = [i for i in range(1, number_of) if holding[i] < largest] or [i for i in range(1, number_of) if holding[i] < reach]
        pool, budget = sum([portions[i] for i in movable]), spare
        for i in movable:
            addition = min(reach - holding[i], max(1, budget * portions[i] // pool), spare)
            holding[i] = holding[i] + addition
            spare = spare - addition
    return np.array(holding)


def noise(rng, extent, deviation, limit, cuts=(), kind=jnp.bfloat16):
    loudness = levels(rng, extent, cuts, -0.22, 0.18) if cuts else 1.0
    array = jax.random.normal(rng, extent, jnp.float32) * deviation * loudness
    return jnp.minimum(jnp.maximum(array, -limit), limit).astype(kind)


def setup_inputs(seed: int = 0) -> dict:
    key_list = jax.random.split(jax.random.key(seed), 17)
    layer_input = noise(key_list[0], (TOKENS, D), 1.0, 6.0, ((0, 32), (1, 16)))
    doc_ids = jnp.searchsorted(jnp.cumsum(uneven_parts(key_list[1], N_SP // 4, TOKENS, 6 * TOK_DEV, 2)), jnp.arange(TOKENS), side="right").astype(jnp.int32)
    routes_keys = jax.random.split(jax.random.fold_in(key_list[2], 1), TOKENS // TOK_DEV)
    routes_turns = jax.random.permutation(jax.random.fold_in(key_list[2], 3), TOKENS // TOK_DEV)
    routes = jax.vmap(lambda own, number: routed_block(jax.random.fold_in(key_list[2], 2), own, number, TOK_DEV, EXPERTS, TOP_K, CAPACITY, 2))(routes_keys, routes_turns).reshape((TOKENS, TOP_K))
    route_weight = jnp.clip(jnp.exp(math.log(2.0) - 2.3025851 * jax.random.uniform(key_list[3], (TOKENS, TOP_K), jnp.float32) ** levels(key_list[3], (TOKENS, TOP_K), ((0, 32),), -0.2, 0.2)), 0.2, 2.0)
    pool_weight = noise(key_list[4], (GROUPS, GROUP_WIDTH, GROUP_WIDTH), GROUP_WIDTH ** -0.5, 0.25)
    pool_scale = jnp.clip(1.0 + 0.18 * jax.random.normal(key_list[5], (D,), jnp.float32), 0.1, 1.9)
    norm1_gain = jnp.clip(jnp.exp(jax.random.uniform(key_list[6], (D,), jnp.float32, math.log(0.3), math.log(3.0))), 0.3, 3.0)
    norm1_bias = noise(key_list[7], (D,), 0.5, 3.0, (), jnp.float32)
    expert_gate = noise(key_list[8], (EXPERTS, D, EXPERT_WIDTH), D ** -0.5, 0.125, ((0, 32), (2, 16)))
    expert_up = noise(key_list[9], (EXPERTS, D, EXPERT_WIDTH), D ** -0.5, 0.125, ((0, 32), (2, 16)))
    expert_down = noise(key_list[10], (EXPERTS, EXPERT_WIDTH, D), EXPERT_WIDTH ** -0.5, 0.125, ((0, 32), (1, 16)))
    shared_gate = noise(key_list[11], (D, SHARED_WIDTH), D ** -0.5, 0.125, ((1, 16),))
    shared_up = noise(key_list[12], (D, SHARED_WIDTH), D ** -0.5, 0.125, ((1, 16),))
    shared_down = noise(key_list[13], (SHARED_WIDTH, D), SHARED_WIDTH ** -0.5, 0.1875, ((0, 16),))
    norm2_gain = jnp.clip(1.0 + 0.18 * jax.random.normal(key_list[14], (D,), jnp.float32), 0.1, 1.9)
    norm2_bias = noise(key_list[15], (D,), 0.5, 3.0, ((0, 16),), jnp.float32)
    return dict(layer_input=layer_input, doc_ids=doc_ids, routes=routes, route_weight=route_weight, pool_weight=pool_weight, pool_scale=pool_scale, norm1_gain=norm1_gain, norm1_bias=norm1_bias, expert_gate=expert_gate, expert_up=expert_up, expert_down=expert_down, shared_gate=shared_gate, shared_up=shared_up, shared_down=shared_down, norm2_gain=norm2_gain, norm2_bias=norm2_bias)


WINDOWS = (2, 4, 8, 16)
HALO_ROWS = 15
RESIDUAL_SCALE = 2.0 ** 0.5
NORM_EPS = 1e-05

def pooled_groups(extended, marks, halo_rows):
    length = extended.shape[0] - halo_rows
    group_width = extended.shape[1] // len(WINDOWS)
    own_mark = marks[halo_rows:]
    values = extended.astype(jnp.float32)
    outputs = []
    for group_index, window in enumerate(WINDOWS):
        section = values[:, group_index * group_width:(group_index + 1) * group_width]
        running = jnp.zeros((length, group_width), jnp.float32)
        members = jnp.zeros((length, 1), jnp.float32)
        for offset in range(window):
            first_row = halo_rows - offset
            inside = (marks[first_row:first_row + length] == own_mark).astype(jnp.float32)[:, None]
            running = running + inside * section[first_row:first_row + length]
            members = members + inside
        outputs.append(running / members - section[halo_rows:])
    return jnp.concatenate(outputs, axis=1).astype(jnp.bfloat16)

def layer_norm_rows(values, gain, bias):
    row_mean = lax.optimization_barrier(jnp.mean(values, axis=1, keepdims=True))
    row_var = lax.optimization_barrier(jnp.mean(values * values, axis=1, keepdims=True)) - row_mean * row_mean
    return (values - row_mean) * lax.rsqrt(row_var + NORM_EPS) * gain + bias

def blockwise_down(hidden, down_weight, pieces):
    piece_width = hidden.shape[1] // pieces

    def add_piece(piece_index, running):
        begin = piece_index.astype(jnp.int32) * piece_width
        part_hidden = lax.dynamic_slice_in_dim(hidden, begin, piece_width, 1)
        part_down = lax.dynamic_slice_in_dim(down_weight, begin, piece_width, 0)
        product = jnp.dot(part_hidden, part_down, preferred_element_type=jnp.float32)
        return running + lax.optimization_barrier(product.astype(jnp.bfloat16)).astype(jnp.float32)
    start_value = jnp.zeros((hidden.shape[0], down_weight.shape[1]), jnp.float32)
    return lax.fori_loop(0, pieces, add_piece, start_value)

def reference(layer_input, doc_ids, routes, route_weight, pool_weight, pool_scale, norm1_gain, norm1_bias, expert_gate, expert_up, expert_down, shared_gate, shared_up, shared_down, norm2_gain, norm2_bias):
    extended = jnp.concatenate([jnp.zeros((HALO_ROWS, D), jnp.bfloat16), layer_input], axis=0)
    marks = jnp.concatenate([jnp.zeros((HALO_ROWS,), jnp.float32), (doc_ids + 1).astype(jnp.float32)])
    mixed = pooled_groups(extended, marks, HALO_ROWS)
    projected = jnp.einsum('tgc,gcd->tgd', mixed.reshape(TOKENS, GROUPS, GROUP_WIDTH).astype(jnp.float32), pool_weight.astype(jnp.float32)).reshape(TOKENS, D)
    first = RESIDUAL_SCALE * layer_input.astype(jnp.float32) + projected * pool_scale
    normed = layer_norm_rows(first, norm1_gain, norm1_bias).astype(jnp.bfloat16)
    picks = routes.reshape(N_SP, TOK_DEV * TOP_K).astype(jnp.int32)
    one_hot = (picks[:, :, None] == jnp.arange(EXPERTS, dtype=jnp.int32)[None, None, :]).astype(jnp.int32)
    ranks = lax.optimization_barrier(jnp.sum((jnp.cumsum(one_hot, axis=1) - one_hot) * one_hot, axis=2)).astype(jnp.int32)
    block_index = jnp.broadcast_to(jnp.arange(N_SP, dtype=jnp.int32)[:, None], picks.shape)
    source_rows = jnp.repeat(normed.reshape(N_SP, TOK_DEV, D), TOP_K, axis=1)
    slots = jnp.zeros((EXPERTS, N_SP, CAPACITY, D), jnp.bfloat16).at[picks, block_index, ranks].set(source_rows)

    def run_expert(operands):
        rows_in, gate_w, up_w, down_w = operands
        slot_rows = rows_in.reshape(N_SP * CAPACITY, D)
        gate_part = jnp.dot(slot_rows, gate_w, preferred_element_type=jnp.float32)
        up_part = jnp.dot(slot_rows, up_w, preferred_element_type=jnp.float32)
        hidden = (jax.nn.silu(gate_part) * up_part).astype(jnp.bfloat16)
        return blockwise_down(hidden, down_w, N_TP).astype(jnp.bfloat16).reshape(N_SP, CAPACITY, D)
    routed = lax.map(run_expert, (slots, expert_gate, expert_up, expert_down))
    returned = routed[picks, block_index, ranks].astype(jnp.float32).reshape(TOKENS, TOP_K, D)
    routed_mix = lax.optimization_barrier(jnp.sum(returned * route_weight[:, :, None], axis=1))
    shared_hidden = (jax.nn.silu(jnp.dot(normed, shared_gate, preferred_element_type=jnp.float32)) * jnp.dot(normed, shared_up, preferred_element_type=jnp.float32)).astype(jnp.bfloat16)
    shared = blockwise_down(shared_hidden, shared_down, N_TP)
    second = RESIDUAL_SCALE * normed.astype(jnp.float32) + routed_mix + shared
    return layer_norm_rows(second, norm2_gain, norm2_bias).astype(jnp.bfloat16)
```

```python
import functools

import jax
import jax.numpy as jnp
from jax import lax
from jax.experimental import pallas as pl
from jax.experimental.pallas import tpu as pltpu
from jax.sharding import Mesh
from jax.sharding import PartitionSpec as P


RESIDUAL_SCALE = 2.0**0.5
NORM_EPS = 1e-05
HALO = 16
F32 = jnp.float32
BF16 = jnp.bfloat16
VMEM = pl.BlockSpec(memory_space=pltpu.VMEM)
HBM = pl.BlockSpec(memory_space=pltpu.HBM)

TOKENS_HERE = 256
EXPERTS = 32
LANES = 128
QUARTER = 512
MODEL = 2048
SLOTS_SENT = 8
SLOTS_USED = 6
ROUTED_ROWS = EXPERTS * SLOTS_USED
SHARED_ROWS = 64
BLOCK_ROWS = 320
UP_AT = 2048
DOWN_AT = 4096
PACKED = DOWN_AT + 16 * BLOCK_ROWS
HALF = PACKED // 2


def iota(shape, dim):
    return lax.broadcasted_iota(jnp.int32, shape, dim)


def side(parts):
    return jnp.concatenate(parts, axis=1)


def four(a):
    return jnp.concatenate([a, a, a, a], axis=1)


def as_column(row):
    return jnp.broadcast_to(row, (LANES, row.shape[1])).T


def chosen(mask):
    return mask.astype(F32).astype(BF16)


def row_stats(values):
    lane = iota((values.shape[0], LANES), 1)
    total = jnp.sum(values, axis=1, keepdims=True)
    squares = jnp.sum(values * values, axis=1, keepdims=True)
    return jnp.where(lane == 0, total, jnp.where(lane == 1, squares, 0.0)).T


def mean_and_scale(total):
    mean = total[0:1] / MODEL
    var = total[1:2] / MODEL - mean * mean
    return as_column(mean), as_column(lax.rsqrt(var + NORM_EPS))


def ranks_of(routes):
    expert = iota((EXPERTS, TOKENS_HERE), 0)
    picks = [routes[k : k + 1] == expert for k in range(2)]
    named = chosen(picks[0] | picks[1])
    earlier = chosen(iota((TOKENS_HERE, TOKENS_HERE), 0) < iota((TOKENS_HERE, TOKENS_HERE), 1))
    counts = jnp.dot(named, earlier, preferred_element_type=F32)
    return [
        jnp.sum(jnp.where(p, counts, 0.0), axis=0, keepdims=True).astype(jnp.int32) for p in picks
    ]


def pack_body(gate, up, down, sgate, sup, sdown, out, cols, sems):
    copies = [
        pltpu.make_async_copy(gate, out.at[pl.ds(0, UP_AT)], sems.at[0]),
        pltpu.make_async_copy(up, out.at[pl.ds(UP_AT, UP_AT)], sems.at[1]),
    ]
    for c in copies:
        c.start()
    for b in range(16):
        at = b * BLOCK_ROWS
        lanes = slice(b * LANES, (b + 1) * LANES)
        cols[at : at + 128, :] = down[:, lanes]
        cols[at + 128 : at + 192, :] = sgate[:, lanes]
        cols[at + 192 : at + 256, :] = sup[:, lanes]
        cols[at + 256 : at + 320, :] = sdown[:, lanes]
    last = pltpu.make_async_copy(cols, out.at[pl.ds(DOWN_AT, 16 * BLOCK_ROWS)], sems.at[2])
    last.start()
    for c in copies:
        c.wait()
    last.wait()


def mixer_body(at, near, halo, docs, weight, scale, first_out, stats_out):
    group = at[0]
    own = side([near[i] for i in range(4)]).astype(F32)
    head = side([halo[i] for i in range(4)]).astype(F32)
    ext = jnp.concatenate([head, own], axis=0)
    marks = jnp.concatenate(
        [halo[4].astype(F32), as_column((docs[...] + 1).astype(F32))], axis=0
    )
    running = ext
    members = jnp.ones(marks.shape, F32)
    for step in range(4):
        by = 1 << step
        on = (group >= step).astype(F32)
        inside = jnp.where(pltpu.roll(marks, by, 0) == marks, on, 0.0)
        running = running + four(inside) * pltpu.roll(running, by, 0)
        members = members + inside * pltpu.roll(members, by, 0)
    mixed = (running / four(members) - ext)[HALO:].astype(BF16)
    projected = jnp.dot(mixed, weight[0], preferred_element_type=F32)
    first = RESIDUAL_SCALE * own + projected * scale[...]
    first_out[...] = first
    stats = row_stats(first)[0:8]
    for i in range(4):
        stats_out[i] = stats


def dispatch_body(at, first, stats, gain, bias, routes, send, shared, own, normed_ref):
    x = at[1]
    mean, inv = mean_and_scale(stats[0] + stats[1] + stats[2] + stats[3])
    normed = ((first[...] - four(mean)) * four(inv) * gain[...] + bias[...]).astype(BF16)
    normed_ref[...] = normed
    named = routes[...]
    dests = []
    for k, rank in enumerate(ranks_of(named)):
        slot = named[k : k + 1] * SLOTS_SENT + (rank >> 2)
        dests.append(jnp.where((rank & 3) == x, slot, -1))
    slot = iota((EXPERTS * SLOTS_SENT, TOKENS_HERE), 0)
    pick = chosen((slot == dests[0]) | (slot == dests[1]))
    send[...] = jnp.dot(pick, normed, preferred_element_type=F32).astype(BF16)
    shared[...] = normed_ref[pl.ds(pl.multiple_of(x * SHARED_ROWS, SHARED_ROWS), SHARED_ROWS), :]
    mine = normed[:, 0:LANES]
    for i in range(1, 4):
        mine = jnp.where(x == i, normed[:, i * LANES : (i + 1) * LANES], mine)
    own[...] = mine


def compact_body(rows, shared, out):
    shape = (ROUTED_ROWS, EXPERTS * SLOTS_SENT)
    came = iota(shape, 1)
    within = came & 7
    goes = SLOTS_USED * (came >> 3) + within
    keep = chosen((iota(shape, 0) == goes) & (within < SLOTS_USED))
    packed = jnp.dot(keep, rows[...], preferred_element_type=F32).astype(BF16)
    tail = shared[...]
    for i in range(4):
        out[i, 0:ROUTED_ROWS, :] = packed
        out[i, ROUTED_ROWS:, :] = tail


def expert_body(rows, w0, w1, w2, w3a, w3b, out, xv, wv, sems):
    def copies_of(c, source, start, size):
        return (source, wv.at[c, pl.ds(start, size)])

    plan = [
        (rows, xv),
        (w0, wv.at[0]),
        (w1, wv.at[1]),
        (w2, wv.at[2]),
        (w3a, wv.at[3, pl.ds(0, HALF)]),
        (w3b, wv.at[3, pl.ds(HALF, HALF)]),
    ]
    copies = [pltpu.make_async_copy(s, d, sems.at[i]) for i, (s, d) in enumerate(plan)]
    for c in copies:
        c.start()
    copies[0].wait()
    tokens = side([xv[i, 0:ROUTED_ROWS, :] for i in range(4)])
    shared = side([xv[i, ROUTED_ROWS:, :] for i in range(4)])

    def block(c, b, low, high):
        at = DOWN_AT + b * BLOCK_ROWS
        return wv[c, at + low : at + high, :]

    hidden = []
    for c in range(4):
        copies[c + 1].wait()
        if c == 3:
            copies[5].wait()
        both = side([wv[c, 0:UP_AT, :], wv[c, UP_AT:DOWN_AT, :]])
        parts = jnp.dot(tokens, both, preferred_element_type=F32)
        hidden.append((jax.nn.silu(parts[:, :LANES]) * parts[:, LANES:]).astype(BF16))
    hidden = side(hidden)
    halves = []
    for low in (128, 192):
        halves.append(
            jnp.concatenate(
                [side([block(c, b, low, low + 64) for b in range(16)]) for c in range(4)], axis=0
            )
        )
    contract = (((1,), (1,)), ((), ()))
    sg = lax.dot_general(shared, halves[0], contract, preferred_element_type=F32)
    su = lax.dot_general(shared, halves[1], contract, preferred_element_type=F32)
    shared_hidden = (jax.nn.silu(sg) * su).astype(BF16)
    for b in range(0, 16, 2):
        down = jnp.concatenate(
            [side([block(c, b, 0, 128), block(c, b + 1, 0, 128)]) for c in range(4)], axis=0
        )
        part = jnp.dot(hidden, down, preferred_element_type=F32).astype(BF16)
        out[b, 0:ROUTED_ROWS, :] = part[:, :LANES]
        out[b + 1, 0:ROUTED_ROWS, :] = part[:, LANES:]
        down = jnp.concatenate(
            [side([block(c, b, 256, 320), block(c, b + 1, 256, 320)]) for c in range(4)], axis=0
        )
        part = jnp.dot(shared_hidden, down, preferred_element_type=F32).astype(BF16)
        out[b, ROUTED_ROWS:, :] = part[:, :LANES]
        out[b + 1, ROUTED_ROWS:, :] = part[:, LANES:]


def return_body(parts, send, shared):
    routed = []
    for x in range(4):
        total = parts[x].astype(F32)
        for y in range(1, 4):
            total = total + parts[4 * y + x].astype(F32)
        routed.append(total[:ROUTED_ROWS].astype(BF16))
        shared[x * SHARED_ROWS : (x + 1) * SHARED_ROWS, :] = total[ROUTED_ROWS:]
    rows = jnp.concatenate(routed, axis=0)
    count = 4 * ROUTED_ROWS
    came = iota((1, count), 1)
    x = (
        (came >= ROUTED_ROWS).astype(jnp.int32)
        + (came >= 2 * ROUTED_ROWS).astype(jnp.int32)
        + (came >= 3 * ROUTED_ROWS).astype(jnp.int32)
    )
    within = came - ROUTED_ROWS * x
    source = (within * 10923) >> 16
    goes = 18 * source + 6 * x + within
    move = chosen(iota((count, count), 0) == goes)
    send[...] = jnp.dot(move, rows, preferred_element_type=F32).astype(BF16)


def combine_body(rows, routes, weight, own, shared, second_out, stats_out):
    named = routes[...]
    scale = weight[...]
    slot = iota((4 * ROUTED_ROWS, TOKENS_HERE), 0)
    taken = jnp.zeros(slot.shape, F32)
    for k, rank in enumerate(ranks_of(named)):
        at = named[k : k + 1] * (4 * SLOTS_USED) + SLOTS_USED * (rank & 3) + (rank >> 2)
        taken = jnp.where(slot == at, scale[k : k + 1], taken)
    high = taken.astype(BF16)
    low = (taken - high.astype(F32)).astype(BF16)
    contract = (((0,), (0,)), ((), ()))
    mix = lax.dot_general(high, rows[...], contract, preferred_element_type=F32)
    mix = mix + lax.dot_general(low, rows[...], contract, preferred_element_type=F32)
    second = RESIDUAL_SCALE * own[...].astype(F32) + mix + shared[...]
    second_out[...] = second
    stats = row_stats(second)[0:2]
    for i in range(16):
        stats_out[i] = stats


def settle_body(second, stats, gain, bias, out):
    total = stats[0]
    for i in range(1, 16):
        total = total + stats[i]
    mean, inv = mean_and_scale(total)
    out[...] = ((second[...] - mean) * inv * gain[...] + bias[...]).astype(BF16)


def struct(shape, dtype):
    return jax.ShapeDtypeStruct(shape, dtype)


def exchange(parts, axes):
    return lax.all_to_all(parts, axes, split_axis=0, concat_axis=0, tiled=True)


def around(shard, by):
    return lax.ppermute(shard, "x", [(i, (i + by) % 4) for i in range(4)])


def shards(
    layer_input,
    doc_ids,
    routes,
    route_weight,
    pool_weight,
    pool_scale,
    norm1_gain,
    norm1_bias,
    expert_gate,
    expert_up,
    expert_down,
    shared_gate,
    shared_up,
    shared_down,
    norm2_gain,
    norm2_bias,
):
    at = jnp.stack([lax.axis_index("y"), lax.axis_index("x")]).astype(jnp.int32)
    near = exchange(jnp.broadcast_to(layer_input, (4, *layer_input.shape)), "x")
    marks = jnp.broadcast_to((doc_ids[-HALO:] + 1).astype(BF16)[:, None], (HALO, LANES))
    tail = jnp.concatenate([near[:, -HALO:, :], marks[None]], axis=0)
    halo = lax.ppermute(tail, "sp", [(i, i + 1) for i in range(lax.axis_size("sp") - 1)])
    packed = pl.pallas_call(
        pack_body,
        out_shape=struct((PACKED, LANES), BF16),
        in_specs=[HBM, HBM, VMEM, VMEM, VMEM, VMEM],
        out_specs=HBM,
        scratch_shapes=[
            pltpu.VMEM((16 * BLOCK_ROWS, LANES), BF16),
            pltpu.SemaphoreType.DMA((3,)),
        ],
        name="pack",
    )(expert_gate[0], expert_up[0], expert_down[0], shared_gate.T, shared_up.T, shared_down)
    packed, halo = lax.optimization_barrier((packed, halo))
    from_left = around(packed, 1)
    from_right = around(packed, -1)
    first, stats = pl.pallas_call(
        mixer_body,
        grid_spec=pltpu.PrefetchScalarGridSpec(
            num_scalar_prefetch=1,
            grid=(1,),
            in_specs=[
                pl.BlockSpec((4, TOKENS_HERE, LANES), lambda i, w: (0, 0, 0)),
                pl.BlockSpec((5, HALO, LANES), lambda i, w: (0, 0, 0)),
                pl.BlockSpec((1, TOKENS_HERE), lambda i, w: (0, 0)),
                pl.BlockSpec((1, QUARTER, QUARTER), lambda i, w: (w[0], 0, 0)),
                pl.BlockSpec((1, QUARTER), lambda i, w: (0, w[0])),
            ],
            out_specs=[
                pl.BlockSpec((TOKENS_HERE, QUARTER), lambda i, w: (0, 0)),
                pl.BlockSpec((4, 8, TOKENS_HERE), lambda i, w: (0, 0, 0)),
            ],
        ),
        out_shape=[
            struct((TOKENS_HERE, QUARTER), F32),
            struct((4, 8, TOKENS_HERE), F32),
        ],
        name="mixer",
    )(at, near, halo, doc_ids[None], pool_weight, pool_scale[None])
    stats = exchange(stats, "y")
    send, shared_rows, own = pl.pallas_call(
        dispatch_body,
        grid_spec=pltpu.PrefetchScalarGridSpec(
            num_scalar_prefetch=1,
            grid=(1,),
            in_specs=[
                pl.BlockSpec((TOKENS_HERE, QUARTER), lambda i, w: (0, 0)),
                pl.BlockSpec((4, 8, TOKENS_HERE), lambda i, w: (0, 0, 0)),
                pl.BlockSpec((1, QUARTER), lambda i, w: (0, w[0])),
                pl.BlockSpec((1, QUARTER), lambda i, w: (0, w[0])),
                pl.BlockSpec((2, TOKENS_HERE), lambda i, w: (0, 0)),
            ],
            out_specs=[
                pl.BlockSpec((EXPERTS * SLOTS_SENT, QUARTER), lambda i, w: (0, 0)),
                pl.BlockSpec((SHARED_ROWS, QUARTER), lambda i, w: (0, 0)),
                pl.BlockSpec((TOKENS_HERE, LANES), lambda i, w: (0, 0)),
            ],
            scratch_shapes=[pltpu.VMEM((TOKENS_HERE, QUARTER), BF16)],
        ),
        out_shape=[
            struct((EXPERTS * SLOTS_SENT, QUARTER), BF16),
            struct((SHARED_ROWS, QUARTER), BF16),
            struct((TOKENS_HERE, LANES), BF16),
        ],
        name="dispatch",
    )(at, first, stats, norm1_gain[None], norm1_bias[None], routes.T)
    arrived = exchange(send.reshape(EXPERTS, SLOTS_SENT, QUARTER), "sp")
    from_left, from_right, arrived = lax.optimization_barrier((from_left, from_right, arrived))
    across_low = around(from_left[:HALF], 1)
    across_high = around(from_right[HALF:], -1)
    gather_in = pl.pallas_call(
        compact_body,
        out_shape=struct((4, TOKENS_HERE, QUARTER), BF16),
        in_specs=[VMEM, VMEM],
        out_specs=VMEM,
        name="compact",
    )(arrived.reshape(EXPERTS * SLOTS_SENT, QUARTER), shared_rows)
    gathered = exchange(gather_in, "y")
    partial = pl.pallas_call(
        expert_body,
        out_shape=struct((16, TOKENS_HERE, LANES), BF16),
        in_specs=[HBM] * 6,
        out_specs=VMEM,
        scratch_shapes=[
            pltpu.VMEM((4, TOKENS_HERE, QUARTER), BF16),
            pltpu.VMEM((4, PACKED, LANES), BF16),
            pltpu.SemaphoreType.DMA((6,)),
        ],
        compiler_params=pltpu.CompilerParams(vmem_limit_bytes=40 * 1024 * 1024),
        name="experts",
    )(gathered, packed, from_left, from_right, across_low, across_high)
    parts = exchange(partial, ("y", "x"))
    back, shared_sum = pl.pallas_call(
        return_body,
        out_shape=[
            struct((4 * ROUTED_ROWS, LANES), BF16),
            struct((TOKENS_HERE, LANES), F32),
        ],
        in_specs=[VMEM],
        out_specs=[VMEM, VMEM],
        name="giveback",
    )(parts)
    returned = exchange(back.reshape(EXPERTS, 4 * SLOTS_USED, LANES), "sp")
    second, row_sums = pl.pallas_call(
        combine_body,
        out_shape=[struct((TOKENS_HERE, LANES), F32), struct((16, 2, TOKENS_HERE), F32)],
        in_specs=[VMEM] * 5,
        out_specs=[VMEM, VMEM],
        name="combine",
    )(returned.reshape(4 * ROUTED_ROWS, LANES), routes.T, route_weight.T, own, shared_sum)
    row_sums = exchange(row_sums, ("y", "x"))
    return pl.pallas_call(
        settle_body,
        out_shape=struct((TOKENS_HERE, LANES), BF16),
        in_specs=[VMEM] * 4,
        out_specs=VMEM,
        name="settle",
    )(second, row_sums, norm2_gain[None], norm2_bias[None])


def solution(mesh):
    split = Mesh(mesh.devices.reshape(mesh.shape["sp"], 4, 4), ("sp", "y", "x"))
    tp = ("y", "x")
    placed = (
        P("sp", tp),
        P("sp"),
        P("sp", None),
        P("sp", None),
        P(),
        P(),
        P(),
        P(),
        P("sp", None, tp),
        P("sp", None, tp),
        P("sp", tp, None),
        P(None, tp),
        P(None, tp),
        P(tp, None),
        P(tp),
        P(tp),
    )
    return jax.shard_map(
        shards, mesh=split, in_specs=placed, out_specs=P("sp", tp), check_vma=False
    )
```

```python
import jax
import jax.numpy as jnp
from jax import lax
from jax.experimental import pallas as pl
from jax.experimental.pallas import tpu as pltpu
from jax.sharding import Mesh
from jax.sharding import PartitionSpec as P


RESIDUAL_SCALE = 2.0**0.5
NORM_EPS = 1e-05
HALO = 16
F32 = jnp.float32
BF16 = jnp.bfloat16
VMEM = pl.BlockSpec(memory_space=pltpu.VMEM)
HBM = pl.BlockSpec(memory_space=pltpu.HBM)

TOKENS_HERE = 256
EXPERTS = 32
LANES = 128
QUARTER = 512
MODEL = 2048
SLOTS_SENT = 8
SLOTS_USED = 6
ROUTED_ROWS = EXPERTS * SLOTS_USED
SHARED_ROWS = 128
UP_AT = 2048
DOWN_AT = 4096
PACKED = 6144
SHARED_UNITS = 64


def iota(shape, dim):
    return lax.broadcasted_iota(jnp.int32, shape, dim)


def side(parts):
    return jnp.concatenate(parts, axis=1)


def four(a):
    return jnp.concatenate([a, a, a, a], axis=1)


def as_column(row):
    return jnp.broadcast_to(row, (LANES, row.shape[1])).T


def chosen(mask):
    return mask.astype(F32).astype(BF16)


def row_stats(values):
    lane = iota((values.shape[0], LANES), 1)
    total = jnp.sum(values, axis=1, keepdims=True)
    squares = jnp.sum(values * values, axis=1, keepdims=True)
    return jnp.where(lane == 0, total, jnp.where(lane == 1, squares, 0.0)).T


def mean_and_scale(total):
    mean = total[0:1] / MODEL
    var = total[1:2] / MODEL - mean * mean
    return as_column(mean), as_column(lax.rsqrt(var + NORM_EPS))


def ranks_of(routes):
    expert = iota((EXPERTS, TOKENS_HERE), 0)
    picks = [routes[k : k + 1] == expert for k in range(2)]
    named = chosen(picks[0] | picks[1])
    earlier = chosen(iota((TOKENS_HERE, TOKENS_HERE), 0) < iota((TOKENS_HERE, TOKENS_HERE), 1))
    counts = jnp.dot(named, earlier, preferred_element_type=F32)
    return [
        jnp.sum(jnp.where(p, counts, 0.0), axis=0, keepdims=True).astype(jnp.int32) for p in picks
    ]


def pack_body(gate, up, down, sgate, sup, sdown, out, shared_out, buf, shared_buf, sems):
    def moves(i):
        here = pl.ds(i * UP_AT, UP_AT)
        return pltpu.make_async_copy((gate, up)[i], buf.at[here], sems.at[i])

    def sends(i):
        here = pl.ds(i * UP_AT, UP_AT)
        return pltpu.make_async_copy(buf.at[here], out.at[here], sems.at[2 + i])

    moves(0).start()
    moves(1).start()
    for b in range(16):
        at = DOWN_AT + b * LANES
        buf[at : at + LANES, :] = down[:, b * LANES : (b + 1) * LANES]
    sends(2).start()
    for i, part in enumerate((sgate, sup, sdown)):
        shared_buf[i * SHARED_UNITS : (i + 1) * SHARED_UNITS, :] = part[...]
    last = pltpu.make_async_copy(shared_buf, shared_out, sems.at[5])
    last.start()
    for i in range(2):
        moves(i).wait()
        sends(i).start()
    for i in range(3):
        sends(i).wait()
    last.wait()


def mixer_body(at, near, halo, docs, weight, scale, first_out, stats_out):
    group = at[0]
    own = side([near[i] for i in range(4)]).astype(F32)
    head = side([halo[i] for i in range(4)]).astype(F32)
    ext = jnp.concatenate([head, own], axis=0)
    marks = jnp.concatenate(
        [halo[4].astype(F32), as_column((docs[...] + 1).astype(F32))], axis=0
    )
    running = ext
    members = jnp.ones(marks.shape, F32)
    for step in range(4):
        by = 1 << step
        on = (group >= step).astype(F32)
        inside = jnp.where(pltpu.roll(marks, by, 0) == marks, on, 0.0)
        running = running + four(inside) * pltpu.roll(running, by, 0)
        members = members + inside * pltpu.roll(members, by, 0)
    mixed = (running / four(members) - ext)[HALO:].astype(BF16)
    projected = jnp.dot(mixed, weight[0], preferred_element_type=F32)
    first = RESIDUAL_SCALE * own + projected * scale[...]
    first_out[...] = first
    stats = row_stats(first)[0:8]
    for i in range(4):
        stats_out[i] = stats


def dispatch_body(at, first, stats, gain, bias, routes, send, normed_out, own):
    x = at[1]
    mean, inv = mean_and_scale(stats[0] + stats[1] + stats[2] + stats[3])
    normed = ((first[...] - four(mean)) * four(inv) * gain[...] + bias[...]).astype(BF16)
    normed_out[...] = normed
    named = routes[...]
    dests = []
    for k, rank in enumerate(ranks_of(named)):
        slot = named[k : k + 1] * SLOTS_SENT + (rank >> 2)
        dests.append(jnp.where((rank & 3) == x, slot, -1))
    slot = iota((EXPERTS * SLOTS_SENT, TOKENS_HERE), 0)
    pick = chosen((slot == dests[0]) | (slot == dests[1]))
    send[...] = jnp.dot(pick, normed, preferred_element_type=F32).astype(BF16)
    mine = normed[:, 0:LANES]
    for i in range(1, 4):
        mine = jnp.where(x == i, normed[:, i * LANES : (i + 1) * LANES], mine)
    own[...] = mine


def compact_body(rows, normed, out):
    shape = (ROUTED_ROWS, EXPERTS * SLOTS_SENT)
    came = iota(shape, 1)
    within = came & 7
    goes = SLOTS_USED * (came >> 3) + within
    keep = chosen((iota(shape, 0) == goes) & (within < SLOTS_USED))
    packed = jnp.dot(keep, rows[...], preferred_element_type=F32).astype(BF16)
    for i in range(4):
        out[i, 0:ROUTED_ROWS, :] = packed
        out[i, ROUTED_ROWS:, :] = normed[(i & 1) * SHARED_ROWS : ((i & 1) + 1) * SHARED_ROWS, :]


def expert_body(rows, w0, w1, w2, w3, s0, s1, out, xv, wv, sv, sems):
    plan = [(rows, xv), (w0, wv.at[0]), (w1, wv.at[1]), (w2, wv.at[2]), (w3, wv.at[3])]
    plan += [(s0, sv.at[0]), (s1, sv.at[1])]
    copies = [pltpu.make_async_copy(s, d, sems.at[i]) for i, (s, d) in enumerate(plan)]
    for c in copies:
        c.start()
    copies[0].wait()
    tokens = side([xv[i, 0:ROUTED_ROWS, :] for i in range(4)])
    hidden = []
    for c in range(4):
        copies[c + 1].wait()
        both = side([wv[c, 0:UP_AT, :], wv[c, UP_AT:DOWN_AT, :]])
        parts = jnp.dot(tokens, both, preferred_element_type=F32)
        hidden.append((jax.nn.silu(parts[:, :LANES]) * parts[:, LANES:]).astype(BF16))
    hidden = side(hidden)
    copies[5].wait()
    copies[6].wait()
    shared = side([xv[i, ROUTED_ROWS:, :] for i in range(4)])

    def units(i, lanes):
        here = slice(i * SHARED_UNITS, (i + 1) * SHARED_UNITS)
        return jnp.concatenate([sv[0, here, lanes], sv[1, here, lanes]], axis=0)

    contract = (((1,), (1,)), ((), ()))
    every = slice(0, MODEL)
    sg = lax.dot_general(shared, units(0, every), contract, preferred_element_type=F32)
    su = lax.dot_general(shared, units(1, every), contract, preferred_element_type=F32)
    shared_hidden = (jax.nn.silu(sg) * su).astype(BF16)

    def block(c, b):
        at = DOWN_AT + b * LANES
        return wv[c, at : at + LANES, :]

    for b in range(0, 16, 2):
        down = jnp.concatenate([side([block(c, b), block(c, b + 1)]) for c in range(4)], axis=0)
        part = jnp.dot(hidden, down, preferred_element_type=F32).astype(BF16)
        out[b, 0:ROUTED_ROWS, :] = part[:, :LANES]
        out[b + 1, 0:ROUTED_ROWS, :] = part[:, LANES:]
        down = units(2, slice(b * LANES, (b + 2) * LANES))
        part = jnp.dot(shared_hidden, down, preferred_element_type=F32).astype(BF16)
        out[b, ROUTED_ROWS:, :] = part[:, :LANES]
        out[b + 1, ROUTED_ROWS:, :] = part[:, LANES:]


def return_body(parts, send, shared):
    routed = []
    for x in range(4):
        total = parts[x, 0:ROUTED_ROWS, :].astype(F32)
        for y in range(1, 4):
            total = total + parts[4 * y + x, 0:ROUTED_ROWS, :].astype(F32)
        routed.append(total.astype(BF16))
    for half in range(2):
        total = jnp.zeros((SHARED_ROWS, LANES), F32)
        for y in (half, half + 2):
            for x in range(4):
                total = total + parts[4 * y + x, ROUTED_ROWS:, :].astype(F32)
        shared[half * SHARED_ROWS : (half + 1) * SHARED_ROWS, :] = total
    rows = jnp.concatenate(routed, axis=0)
    count = 4 * ROUTED_ROWS
    came = iota((1, count), 1)
    x = (
        (came >= ROUTED_ROWS).astype(jnp.int32)
        + (came >= 2 * ROUTED_ROWS).astype(jnp.int32)
        + (came >= 3 * ROUTED_ROWS).astype(jnp.int32)
    )
    within = came - ROUTED_ROWS * x
    source = (within * 10923) >> 16
    goes = 18 * source + 6 * x + within
    move = chosen(iota((count, count), 0) == goes)
    send[...] = jnp.dot(move, rows, preferred_element_type=F32).astype(BF16)


def combine_body(rows, routes, weight, own, shared, second_out, stats_out):
    named = routes[...]
    scale = weight[...]
    slot = iota((4 * ROUTED_ROWS, TOKENS_HERE), 0)
    taken = jnp.zeros(slot.shape, F32)
    for k, rank in enumerate(ranks_of(named)):
        at = named[k : k + 1] * (4 * SLOTS_USED) + SLOTS_USED * (rank & 3) + (rank >> 2)
        taken = jnp.where(slot == at, scale[k : k + 1], taken)
    high = taken.astype(BF16)
    low = (taken - high.astype(F32)).astype(BF16)
    contract = (((0,), (0,)), ((), ()))
    mix = lax.dot_general(high, rows[...], contract, preferred_element_type=F32)
    mix = mix + lax.dot_general(low, rows[...], contract, preferred_element_type=F32)
    second = RESIDUAL_SCALE * own[...].astype(F32) + mix + shared[...]
    second_out[...] = second
    stats = row_stats(second)[0:2]
    for i in range(16):
        stats_out[i] = stats


def settle_body(second, stats, gain, bias, out):
    total = stats[0]
    for i in range(1, 16):
        total = total + stats[i]
    mean, inv = mean_and_scale(total)
    out[...] = ((second[...] - mean) * inv * gain[...] + bias[...]).astype(BF16)


def struct(shape, dtype):
    return jax.ShapeDtypeStruct(shape, dtype)


def exchange(parts, axes):
    return lax.all_to_all(parts, axes, split_axis=0, concat_axis=0, tiled=True)


def around(shard, by):
    return lax.ppermute(shard, "x", [(i, (i + by) % 4) for i in range(4)])


def kernel(body, **options):
    return pl.pallas_call(body, **options)


def layer(
    layer_input,
    doc_ids,
    routes,
    route_weight,
    pool_weight,
    pool_scale,
    norm1_gain,
    norm1_bias,
    expert_gate,
    expert_up,
    expert_down,
    shared_gate,
    shared_up,
    shared_down,
    norm2_gain,
    norm2_bias,
):
    at = jnp.stack([lax.axis_index("y"), lax.axis_index("x")]).astype(jnp.int32)
    near = exchange(jnp.broadcast_to(layer_input, (4, *layer_input.shape)), "x")
    packed, shared_packed = kernel(
        pack_body,
        out_shape=[struct((PACKED, LANES), BF16), struct((3 * SHARED_UNITS, MODEL), BF16)],
        in_specs=[HBM, HBM, VMEM, VMEM, VMEM, VMEM],
        out_specs=[HBM, HBM],
        scratch_shapes=[
            pltpu.VMEM((PACKED, LANES), BF16),
            pltpu.VMEM((3 * SHARED_UNITS, MODEL), BF16),
            pltpu.SemaphoreType.DMA((6,)),
        ],
        cost_estimate=pl.CostEstimate(
            flops=10_000_000, bytes_accessed=4 * PACKED * LANES, transcendentals=0
        ),
    )(expert_gate[0], expert_up[0], expert_down[0], shared_gate.T, shared_up.T, shared_down)
    packed, shared_packed, near = lax.optimization_barrier((packed, shared_packed, near))
    marks = jnp.broadcast_to((doc_ids[-HALO:] + 1).astype(BF16)[:, None], (HALO, LANES))
    tail = jnp.concatenate([near[:, -HALO:, :], marks[None]], axis=0)
    following = [(i, i + 1) for i in range(lax.axis_size("sp") - 1)]
    halo = lax.ppermute(tail, "sp", following)
    from_left = around(packed, 1)
    from_right = around(packed, -1)
    first, stats = kernel(
        mixer_body,
        grid_spec=pltpu.PrefetchScalarGridSpec(
            num_scalar_prefetch=1,
            grid=(1,),
            in_specs=[
                pl.BlockSpec((4, TOKENS_HERE, LANES), lambda i, w: (0, 0, 0)),
                pl.BlockSpec((5, HALO, LANES), lambda i, w: (0, 0, 0)),
                pl.BlockSpec((1, TOKENS_HERE), lambda i, w: (0, 0)),
                pl.BlockSpec((1, QUARTER, QUARTER), lambda i, w: (w[0], 0, 0)),
                pl.BlockSpec((1, QUARTER), lambda i, w: (0, w[0])),
            ],
            out_specs=[
                pl.BlockSpec((TOKENS_HERE, QUARTER), lambda i, w: (0, 0)),
                pl.BlockSpec((4, 8, TOKENS_HERE), lambda i, w: (0, 0, 0)),
            ],
        ),
        out_shape=[
            struct((TOKENS_HERE, QUARTER), F32),
            struct((4, 8, TOKENS_HERE), F32),
        ],
    )(at, near, halo, doc_ids[None], pool_weight, pool_scale[None])
    later, first = lax.optimization_barrier((packed, first))
    from_across = around(later, 2)
    stats = exchange(stats, "y")
    send, normed, own = kernel(
        dispatch_body,
        grid_spec=pltpu.PrefetchScalarGridSpec(
            num_scalar_prefetch=1,
            grid=(1,),
            in_specs=[
                pl.BlockSpec((TOKENS_HERE, QUARTER), lambda i, w: (0, 0)),
                pl.BlockSpec((4, 8, TOKENS_HERE), lambda i, w: (0, 0, 0)),
                pl.BlockSpec((1, QUARTER), lambda i, w: (0, w[0])),
                pl.BlockSpec((1, QUARTER), lambda i, w: (0, w[0])),
                pl.BlockSpec((2, TOKENS_HERE), lambda i, w: (0, 0)),
            ],
            out_specs=[
                pl.BlockSpec((EXPERTS * SLOTS_SENT, QUARTER), lambda i, w: (0, 0)),
                pl.BlockSpec((TOKENS_HERE, QUARTER), lambda i, w: (0, 0)),
                pl.BlockSpec((TOKENS_HERE, LANES), lambda i, w: (0, 0)),
            ],
        ),
        out_shape=[
            struct((EXPERTS * SLOTS_SENT, QUARTER), BF16),
            struct((TOKENS_HERE, QUARTER), BF16),
            struct((TOKENS_HERE, LANES), BF16),
        ],
    )(at, first, stats, norm1_gain[None], norm1_bias[None], routes.T)
    shared_later, send = lax.optimization_barrier((shared_packed, send))
    from_pair = lax.ppermute(shared_later, "y", [(i, i ^ 1) for i in range(4)])
    arrived = exchange(send.reshape(EXPERTS, SLOTS_SENT, QUARTER), "sp")
    gather_in = kernel(
        compact_body,
        out_shape=struct((4, ROUTED_ROWS + SHARED_ROWS, QUARTER), BF16),
        in_specs=[VMEM, VMEM],
        out_specs=VMEM,
    )(arrived.reshape(EXPERTS * SLOTS_SENT, QUARTER), normed)
    gathered = exchange(gather_in, "y")
    partial = kernel(
        expert_body,
        out_shape=struct((16, ROUTED_ROWS + SHARED_ROWS, LANES), BF16),
        in_specs=[HBM] * 7,
        out_specs=VMEM,
        scratch_shapes=[
            pltpu.VMEM((4, ROUTED_ROWS + SHARED_ROWS, QUARTER), BF16),
            pltpu.VMEM((4, PACKED, LANES), BF16),
            pltpu.VMEM((2, 3 * SHARED_UNITS, MODEL), BF16),
            pltpu.SemaphoreType.DMA((7,)),
        ],
        compiler_params=pltpu.CompilerParams(vmem_limit_bytes=40 * 1024 * 1024),
    )(gathered, packed, from_left, from_right, from_across, shared_packed, from_pair)
    parts = exchange(partial, ("y", "x"))
    back, shared_sum = kernel(
        return_body,
        out_shape=[
            struct((4 * ROUTED_ROWS, LANES), BF16),
            struct((TOKENS_HERE, LANES), F32),
        ],
        in_specs=[VMEM],
        out_specs=[VMEM, VMEM],
    )(parts)
    returned = exchange(back.reshape(EXPERTS, 4 * SLOTS_USED, LANES), "sp")
    second, row_sums = kernel(
        combine_body,
        out_shape=[struct((TOKENS_HERE, LANES), F32), struct((16, 2, TOKENS_HERE), F32)],
        in_specs=[VMEM] * 5,
        out_specs=[VMEM, VMEM],
    )(returned.reshape(4 * ROUTED_ROWS, LANES), routes.T, route_weight.T, own, shared_sum)
    row_sums = exchange(row_sums, ("y", "x"))
    return kernel(
        settle_body,
        out_shape=struct((TOKENS_HERE, LANES), BF16),
        in_specs=[VMEM] * 4,
        out_specs=VMEM,
    )(second, row_sums, norm2_gain[None], norm2_bias[None])


def solution(mesh):
    split = Mesh(mesh.devices.reshape(mesh.shape["sp"], 4, 4), ("sp", "y", "x"))
    tp = ("y", "x")
    placed = (
        P("sp", tp),
        P("sp"),
        P("sp", None),
        P("sp", None),
        P(),
        P(),
        P(),
        P(),
        P("sp", None, tp),
        P("sp", None, tp),
        P("sp", tp, None),
        P(None, tp),
        P(None, tp),
        P(tp, None),
        P(tp),
        P(tp),
    )
    return jax.shard_map(layer, mesh=split, in_specs=placed, out_specs=P("sp", tp), check_vma=False)
```

```python
import jax
import jax.numpy as jnp
from jax import lax
from jax.experimental import pallas as pl
from jax.experimental.pallas import tpu as pltpu
from jax.sharding import Mesh
from jax.sharding import PartitionSpec as P


RESIDUAL_SCALE = 2.0**0.5
NORM_EPS = 1e-05
HALO = 16
F32 = jnp.float32
BF16 = jnp.bfloat16
VMEM = pl.BlockSpec(memory_space=pltpu.VMEM)
HELD = pl.BlockSpec(memory_space=pltpu.VMEM)
HBM = pl.BlockSpec(memory_space=pltpu.HBM)
SMEM = pl.BlockSpec(memory_space=pltpu.SMEM)

TOKENS_HERE = 256
EXPERTS = 32
LANES = 128
QUARTER = 512
MODEL = 2048
SLOTS_SENT = 8
SLOTS_USED = 6
ROUTED_ROWS = EXPERTS * SLOTS_USED
SHARED_ROWS = 128
UP_AT = 2048
DOWN_AT = 4096
PACKED = 6144
SHARED_UNITS = 64
RELAYED = PACKED // 2


def iota(shape, dim):
    return lax.broadcasted_iota(jnp.int32, shape, dim)


def side(parts):
    return jnp.concatenate(parts, axis=1)


def four(a):
    return jnp.concatenate([a, a, a, a], axis=1)


def as_column(row):
    return jnp.broadcast_to(row, (LANES, row.shape[1])).T


def chosen(mask):
    return mask.astype(F32).astype(BF16)


def sums(values):
    total = jnp.sum(values, axis=1, keepdims=True)
    return total, jnp.sum(values * values, axis=1, keepdims=True)


def row_stats(values):
    lane = iota((values.shape[0], LANES), 1)
    total, squares = sums(values)
    return jnp.where(lane == 0, total, jnp.where(lane == 1, squares, 0.0)).T


def mean_and_scale(total):
    mean = total[0:1] / MODEL
    var = total[1:2] / MODEL - mean * mean
    return as_column(mean), as_column(lax.rsqrt(var + NORM_EPS))


def ranks_of(routes):
    expert = iota((EXPERTS, TOKENS_HERE), 0)
    picks = [routes[k : k + 1] == expert for k in range(2)]
    named = chosen(picks[0] | picks[1])
    earlier = chosen(iota((TOKENS_HERE, TOKENS_HERE), 0) < iota((TOKENS_HERE, TOKENS_HERE), 1))
    counts = jnp.dot(named, earlier, preferred_element_type=F32)
    return [
        jnp.sum(jnp.where(p, counts, 0.0), axis=0, keepdims=True).astype(jnp.int32) for p in picks
    ]


def pack_body(gate, up, down, sgate, sup, sdown, low, high, shared_out, buf, shared_buf, sems):
    def moves(i):
        here = pl.ds(i * UP_AT, UP_AT)
        return pltpu.make_async_copy((gate, up)[i], buf.at[here], sems.at[i])

    def sends(i):
        here = pl.ds(i * RELAYED, RELAYED)
        return pltpu.make_async_copy(buf.at[here], (low, high)[i], sems.at[2 + i])

    moves(0).start()
    moves(1).start()
    for b in range(16):
        at = DOWN_AT + b * LANES
        buf[at : at + LANES, :] = down[:, b * LANES : (b + 1) * LANES]
    for i, part in enumerate((sgate, sup, sdown)):
        shared_buf[i * SHARED_UNITS : (i + 1) * SHARED_UNITS, :] = part[...]
    last = pltpu.make_async_copy(shared_buf, shared_out, sems.at[4])
    moves(0).wait()
    moves(1).wait()
    sends(0).start()
    sends(1).start()
    last.start()
    sends(0).wait()
    sends(1).wait()
    last.wait()


def spread_body(shard, out):
    for i in range(16):
        out[i] = shard[...]


def mixer_body(
    at,
    docs,
    routes,
    scale,
    gain,
    bias,
    near,
    halo,
    weight,
    send,
    normed,
    own,
    weight_v,
    first_v,
    sems,
):
    y, x = at[0], at[1]
    copies = [pltpu.make_async_copy(weight.at[g], weight_v.at[g], sems.at[g]) for g in range(4)]
    for c in copies:
        c.start()
    marks = jnp.concatenate(
        [halo[16].astype(F32), as_column((docs[...] + 1).astype(F32))], axis=0
    )
    members = jnp.ones(marks.shape, F32)
    insides, counts = [], []
    for step in range(4):
        inside = jnp.where(pltpu.roll(marks, 1 << step, 0) == marks, 1.0, 0.0)
        members = members + inside * pltpu.roll(members, 1 << step, 0)
        insides.append(four(inside))
        counts.append(four(members[HALO:]))
    total = jnp.zeros((TOKENS_HERE, 1), F32)
    squares = jnp.zeros((TOKENS_HERE, 1), F32)
    for g in range(4):
        lanes = slice(g * QUARTER, (g + 1) * QUARTER)
        head = side([halo[4 * g + i] for i in range(4)]).astype(F32)
        mine = side([near[4 * g + i] for i in range(4)]).astype(F32)
        running = jnp.concatenate([head, mine], axis=0)
        for step in range(g + 1):
            running = running + insides[step] * pltpu.roll(running, 1 << step, 0)
        mixed = (running[HALO:] / counts[g] - mine).astype(BF16)
        copies[g].wait()
        projected = jnp.dot(mixed, weight_v[g], preferred_element_type=F32)
        first = RESIDUAL_SCALE * mine + projected * scale[:, lanes]
        first_v[g] = first
        part, part_squares = sums(first)
        total = total + part
        squares = squares + part_squares
    mean = total / MODEL
    inv = lax.rsqrt(squares / MODEL - mean * mean + NORM_EPS)
    for g in range(4):
        lanes = slice(g * QUARTER, (g + 1) * QUARTER)
        normed[g] = ((first_v[g] - mean) * inv * gain[:, lanes] + bias[:, lanes]).astype(BF16)
    quarter = normed[y]
    named = routes[...]
    dests = []
    for k, rank in enumerate(ranks_of(named)):
        slot = named[k : k + 1] * SLOTS_SENT + (rank >> 2)
        dests.append(jnp.where((rank & 3) == x, slot, -1))
    slot = iota((EXPERTS * SLOTS_SENT, TOKENS_HERE), 0)
    pick = chosen((slot == dests[0]) | (slot == dests[1]))
    send[...] = jnp.dot(pick, quarter, preferred_element_type=F32).astype(BF16)
    mine = quarter[:, 0:LANES]
    for i in range(1, 4):
        mine = jnp.where(x == i, quarter[:, i * LANES : (i + 1) * LANES], mine)
    own[...] = mine


def compact_body(rows, out):
    shape = (ROUTED_ROWS, EXPERTS * SLOTS_SENT)
    came = iota(shape, 1)
    within = came & 7
    goes = SLOTS_USED * (came >> 3) + within
    keep = chosen((iota(shape, 0) == goes) & (within < SLOTS_USED))
    packed = jnp.dot(keep, rows[...], preferred_element_type=F32).astype(BF16)
    for i in range(4):
        out[i] = packed


def expert_body(
    at, rows, normed, *rest
):
    shards, (s0, s1, out, nv, wv, sv, sems) = rest[:8], rest[8:]
    half = pl.multiple_of((at[0] & 1) * SHARED_ROWS, SHARED_ROWS)
    plan = [
        (shard, wv.at[i // 2, pl.ds(i % 2 * RELAYED, RELAYED)]) for i, shard in enumerate(shards)
    ]
    plan += [
        (s0, sv.at[0]),
        (s1, sv.at[1]),
        (normed.at[:, pl.ds(half, SHARED_ROWS), :], nv),
    ]
    copies = [pltpu.make_async_copy(s, d, sems.at[i]) for i, (s, d) in enumerate(plan)]
    for c in copies:
        c.start()
    tokens = side([rows[i] for i in range(4)])
    hidden = []
    for c in range(4):
        copies[2 * c].wait()
        copies[2 * c + 1].wait()
        both = side([wv[c, 0:UP_AT, :], wv[c, UP_AT:DOWN_AT, :]])
        parts = jnp.dot(tokens, both, preferred_element_type=F32)
        hidden.append((jax.nn.silu(parts[:, :LANES]) * parts[:, LANES:]).astype(BF16))
    hidden = side(hidden)
    for c in copies[8:]:
        c.wait()
    shared = side([nv[i] for i in range(4)])

    def units(i, lanes):
        here = slice(i * SHARED_UNITS, (i + 1) * SHARED_UNITS)
        return jnp.concatenate([sv[0, here, lanes], sv[1, here, lanes]], axis=0)

    contract = (((1,), (1,)), ((), ()))
    every = slice(0, MODEL)
    sg = lax.dot_general(shared, units(0, every), contract, preferred_element_type=F32)
    su = lax.dot_general(shared, units(1, every), contract, preferred_element_type=F32)
    shared_hidden = (jax.nn.silu(sg) * su).astype(BF16)

    def block(c, b):
        at = DOWN_AT + b * LANES
        return wv[c, at : at + LANES, :]

    for b in range(0, 16, 2):
        down = jnp.concatenate([side([block(c, b), block(c, b + 1)]) for c in range(4)], axis=0)
        part = jnp.dot(hidden, down, preferred_element_type=F32).astype(BF16)
        out[b, 0:ROUTED_ROWS, :] = part[:, :LANES]
        out[b + 1, 0:ROUTED_ROWS, :] = part[:, LANES:]
        down = units(2, slice(b * LANES, (b + 2) * LANES))
        part = jnp.dot(shared_hidden, down, preferred_element_type=F32).astype(BF16)
        out[b, ROUTED_ROWS:, :] = part[:, :LANES]
        out[b + 1, ROUTED_ROWS:, :] = part[:, LANES:]


def return_body(parts, send, shared):
    routed = []
    for x in range(4):
        total = parts[x, 0:ROUTED_ROWS, :].astype(F32)
        for y in range(1, 4):
            total = total + parts[4 * y + x, 0:ROUTED_ROWS, :].astype(F32)
        routed.append(total.astype(BF16))
    for half in range(2):
        total = jnp.zeros((SHARED_ROWS, LANES), F32)
        for y in (half, half + 2):
            for x in range(4):
                total = total + parts[4 * y + x, ROUTED_ROWS:, :].astype(F32)
        shared[half * SHARED_ROWS : (half + 1) * SHARED_ROWS, :] = total
    rows = jnp.concatenate(routed, axis=0)
    count = 4 * ROUTED_ROWS
    came = iota((1, count), 1)
    x = (
        (came >= ROUTED_ROWS).astype(jnp.int32)
        + (came >= 2 * ROUTED_ROWS).astype(jnp.int32)
        + (came >= 3 * ROUTED_ROWS).astype(jnp.int32)
    )
    within = came - ROUTED_ROWS * x
    source = (within * 10923) >> 16
    goes = 18 * source + 6 * x + within
    move = chosen(iota((count, count), 0) == goes)
    send[...] = jnp.dot(move, rows, preferred_element_type=F32).astype(BF16)


def combine_body(rows, routes, weight, own, shared, second_out, stats_out):
    named = routes[...]
    scale = weight[...]
    slot = iota((4 * ROUTED_ROWS, TOKENS_HERE), 0)
    taken = jnp.zeros(slot.shape, F32)
    for k, rank in enumerate(ranks_of(named)):
        at = named[k : k + 1] * (4 * SLOTS_USED) + SLOTS_USED * (rank & 3) + (rank >> 2)
        taken = jnp.where(slot == at, scale[k : k + 1], taken)
    high = taken.astype(BF16)
    low = (taken - high.astype(F32)).astype(BF16)
    contract = (((0,), (0,)), ((), ()))
    mix = lax.dot_general(high, rows[...], contract, preferred_element_type=F32)
    mix = mix + lax.dot_general(low, rows[...], contract, preferred_element_type=F32)
    second = RESIDUAL_SCALE * own[...].astype(F32) + mix + shared[...]
    second_out[...] = second
    stats = row_stats(second)[0:2]
    for i in range(16):
        stats_out[i] = stats


def settle_body(second, stats, gain, bias, out):
    total = stats[0]
    for i in range(1, 16):
        total = total + stats[i]
    mean, inv = mean_and_scale(total)
    out[...] = ((second[...] - mean) * inv * gain[...] + bias[...]).astype(BF16)


def struct(shape, dtype):
    return pltpu.HBM(shape, dtype)


def exchange(parts, axes):
    return lax.all_to_all(parts, axes, split_axis=0, concat_axis=0, tiled=True)


def around(shard, by):
    return lax.ppermute(shard, "x", [(i, (i + by) % 4) for i in range(4)])


def kernel(body, in_specs, **options):
    call = pl.pallas_call(body, in_specs=in_specs, **options)
    places = {id(HELD): pltpu.VMEM, id(HBM): pltpu.HBM}

    def run(*args):
        args = [
            pltpu.with_memory_space_constraint(a, places[id(s)]) if id(s) in places else a
            for a, s in zip(args, in_specs, strict=True)
        ]
        return call(*args)

    return run


def layer(
    layer_input,
    doc_ids,
    routes,
    route_weight,
    pool_weight,
    pool_scale,
    norm1_gain,
    norm1_bias,
    expert_gate,
    expert_up,
    expert_down,
    shared_gate,
    shared_up,
    shared_down,
    norm2_gain,
    norm2_bias,
):
    at = jnp.stack([lax.axis_index("y"), lax.axis_index("x")]).astype(jnp.int32)
    spread = kernel(
        spread_body,
        out_shape=struct((16, TOKENS_HERE, LANES), BF16),
        in_specs=[VMEM],
        out_specs=VMEM,
    )(layer_input)
    near = exchange(spread, ("y", "x"))
    low, high, shared_packed = kernel(
        pack_body,
        out_shape=[
            struct((RELAYED, LANES), BF16),
            struct((RELAYED, LANES), BF16),
            struct((3 * SHARED_UNITS, MODEL), BF16),
        ],
        in_specs=[HBM, HBM, VMEM, VMEM, VMEM, VMEM],
        out_specs=[HBM] * 3,
        scratch_shapes=[
            pltpu.VMEM((PACKED, LANES), BF16),
            pltpu.VMEM((3 * SHARED_UNITS, MODEL), BF16),
            pltpu.SemaphoreType.DMA((5,)),
        ],
        cost_estimate=pl.CostEstimate(
            flops=10_000_000, bytes_accessed=4 * PACKED * LANES, transcendentals=0
        ),
    )(expert_gate[0], expert_up[0], expert_down[0], shared_gate.T, shared_up.T, shared_down)
    marks = jnp.broadcast_to((doc_ids[-HALO:] + 1).astype(BF16)[:, None], (HALO, LANES))
    tail = jnp.concatenate([near[:, -HALO:, :], marks[None]], axis=0)
    following = [(i, i + 1) for i in range(lax.axis_size("sp") - 1)]
    halo = lax.ppermute(tail, "sp", following)
    left_low = around(low, 1)
    right_high = around(high, -1)
    left_high = around(high, 1)
    right_low = around(low, -1)
    send, normed, own = kernel(
        mixer_body,
        in_specs=[SMEM] + [VMEM] * 5 + [HELD, HELD, HBM],
        out_specs=[VMEM] * 3,
        scratch_shapes=[
            pltpu.VMEM((4, QUARTER, QUARTER), BF16),
            pltpu.VMEM((4, TOKENS_HERE, QUARTER), F32),
            pltpu.SemaphoreType.DMA((4,)),
        ],
        out_shape=[
            struct((EXPERTS * SLOTS_SENT, QUARTER), BF16),
            struct((4, TOKENS_HERE, QUARTER), BF16),
            struct((TOKENS_HERE, LANES), BF16),
        ],
        compiler_params=pltpu.CompilerParams(vmem_limit_bytes=40 * 1024 * 1024),
    )(
        at,
        doc_ids[None],
        routes.T,
        pool_scale[None],
        norm1_gain[None],
        norm1_bias[None],
        near,
        halo,
        pool_weight,
    )
    shared_later, send = lax.optimization_barrier((shared_packed, send))
    from_pair = lax.ppermute(shared_later, "y", [(i, i ^ 1) for i in range(4)])
    across_low = around(left_low, 1)
    across_high = around(right_high, -1)
    arrived = exchange(send.reshape(EXPERTS, SLOTS_SENT, QUARTER), "sp")
    gather_in = kernel(
        compact_body,
        out_shape=struct((4, ROUTED_ROWS, QUARTER), BF16),
        in_specs=[HELD],
        out_specs=VMEM,
    )(arrived.reshape(EXPERTS * SLOTS_SENT, QUARTER))
    gathered = exchange(gather_in, "y")
    partial = kernel(
        expert_body,
        out_shape=struct((16, ROUTED_ROWS + SHARED_ROWS, LANES), BF16),
        in_specs=[SMEM, HELD] + [HBM] * 11,
        out_specs=VMEM,
        scratch_shapes=[
            pltpu.VMEM((4, SHARED_ROWS, QUARTER), BF16),
            pltpu.VMEM((4, PACKED, LANES), BF16),
            pltpu.VMEM((2, 3 * SHARED_UNITS, MODEL), BF16),
            pltpu.SemaphoreType.DMA((11,)),
        ],
        compiler_params=pltpu.CompilerParams(vmem_limit_bytes=40 * 1024 * 1024),
    )(
        at,
        gathered,
        normed,
        low,
        high,
        left_low,
        left_high,
        right_low,
        right_high,
        across_low,
        across_high,
        shared_packed,
        from_pair,
    )
    parts = exchange(partial, ("y", "x"))
    back, shared_sum = kernel(
        return_body,
        out_shape=[
            struct((4 * ROUTED_ROWS, LANES), BF16),
            struct((TOKENS_HERE, LANES), F32),
        ],
        in_specs=[HELD],
        out_specs=[VMEM, VMEM],
    )(parts)
    returned = exchange(back.reshape(EXPERTS, 4 * SLOTS_USED, LANES), "sp")
    second, row_sums = kernel(
        combine_body,
        out_shape=[struct((TOKENS_HERE, LANES), F32), struct((16, 2, TOKENS_HERE), F32)],
        in_specs=[HELD] + [VMEM] * 4,
        out_specs=[VMEM, VMEM],
    )(returned.reshape(4 * ROUTED_ROWS, LANES), routes.T, route_weight.T, own, shared_sum)
    row_sums = exchange(row_sums, ("y", "x"))
    return kernel(
        settle_body,
        out_shape=jax.ShapeDtypeStruct((TOKENS_HERE, LANES), BF16),
        in_specs=[VMEM, HELD, VMEM, VMEM],
        out_specs=VMEM,
    )(second, row_sums, norm2_gain[None], norm2_bias[None])


def solution(mesh):
    split = Mesh(mesh.devices.reshape(mesh.shape["sp"], 4, 4), ("sp", "y", "x"))
    tp = ("y", "x")
    placed = (
        P("sp", tp),
        P("sp"),
        P("sp", None),
        P("sp", None),
        P(),
        P(),
        P(),
        P(),
        P("sp", None, tp),
        P("sp", None, tp),
        P("sp", tp, None),
        P(None, tp),
        P(None, tp),
        P(tp, None),
        P(tp),
        P(tp),
    )
    return jax.shard_map(layer, mesh=split, in_specs=placed, out_specs=P("sp", tp), check_vma=False)
```

```python
import jax
import jax.numpy as jnp
from jax import lax
from jax.experimental import pallas as pl
from jax.experimental.pallas import tpu as pltpu
from jax.sharding import Mesh
from jax.sharding import PartitionSpec as P


RESIDUAL_SCALE = 2.0**0.5
NORM_EPS = 1e-05
HALO = 16
F32 = jnp.float32
BF16 = jnp.bfloat16
VMEM = pl.BlockSpec(memory_space=pltpu.VMEM)
HELD = pl.BlockSpec(memory_space=pltpu.VMEM)
HBM = pl.BlockSpec(memory_space=pltpu.HBM)
ANY = pl.BlockSpec(memory_space=pl.ANY)
SMEM = pl.BlockSpec(memory_space=pltpu.SMEM)

TOKENS_HERE = 256
EXPERTS = 32
LANES = 128
QUARTER = 512
MODEL = 2048
SLOTS_SENT = 8
SLOTS_USED = 6
ROUTED_ROWS = EXPERTS * SLOTS_USED
SHARED_ROWS = 128
UP_AT = 2048
DOWN_AT = 4096
PACKED = 6144
SHARED_UNITS = 64
HALF_UNITS = SHARED_UNITS // 2
RELAYED = PACKED // 2


def iota(shape, dim):
    return lax.broadcasted_iota(jnp.int32, shape, dim)


def side(parts):
    return jnp.concatenate(parts, axis=1)


def four(a):
    return jnp.concatenate([a, a, a, a], axis=1)


def as_column(row):
    return jnp.broadcast_to(row, (LANES, row.shape[1])).T


def chosen(mask):
    return mask.astype(F32).astype(BF16)


def sums(values):
    total = jnp.sum(values, axis=1, keepdims=True)
    return total, jnp.sum(values * values, axis=1, keepdims=True)


def row_stats(values):
    lane = iota((values.shape[0], LANES), 1)
    total, squares = sums(values)
    return jnp.where(lane == 0, total, jnp.where(lane == 1, squares, 0.0)).T


def mean_and_scale(total):
    mean = total[0:1] / MODEL
    var = total[1:2] / MODEL - mean * mean
    return as_column(mean), as_column(lax.rsqrt(var + NORM_EPS))


def ranks_of(routes):
    expert = iota((EXPERTS, TOKENS_HERE), 0)
    picks = [routes[k : k + 1] == expert for k in range(2)]
    named = chosen(picks[0] | picks[1])
    earlier = chosen(iota((TOKENS_HERE, TOKENS_HERE), 0) < iota((TOKENS_HERE, TOKENS_HERE), 1))
    counts = jnp.dot(named, earlier, preferred_element_type=F32)
    return [
        jnp.sum(jnp.where(p, counts, 0.0), axis=0, keepdims=True).astype(jnp.int32) for p in picks
    ]


def pack_body(at, gate, up, down, sgate, sup, sdown, low, high, shared_out, half_out, sems):
    core = pl.multiple_of(at[2] * HALF_UNITS, HALF_UNITS)
    rest = DOWN_AT - RELAYED
    plan = [
        (gate, low.at[pl.ds(0, UP_AT)]),
        (up.at[pl.ds(0, RELAYED - UP_AT)], low.at[pl.ds(UP_AT, RELAYED - UP_AT)]),
        (up.at[pl.ds(RELAYED - UP_AT, rest)], high.at[pl.ds(0, rest)]),
    ]
    for b in range(16):
        lanes = pl.ds(b * LANES, LANES)
        plan.append((down.at[:, lanes], high.at[pl.ds(rest + b * LANES, LANES)]))
    for i, part in enumerate((sgate, sup, sdown)):
        plan.append((part, shared_out.at[pl.ds(i * SHARED_UNITS, SHARED_UNITS)]))
        mine = part.at[pl.ds(core, HALF_UNITS)]
        plan.append((mine, half_out.at[pl.ds(i * HALF_UNITS, HALF_UNITS)]))
    copies = [pltpu.make_async_copy(s, d, sems.at[i]) for i, (s, d) in enumerate(plan)]
    for c in copies:
        c.start()
    for c in copies:
        c.wait()


def spread_body(shard, out, block, sems):
    move = pltpu.make_async_copy(shard, block, sems.at[16])
    move.start()
    move.wait()
    copies = [pltpu.make_async_copy(block, out.at[i], sems.at[i]) for i in range(16)]
    for c in copies:
        c.start()
    for c in copies:
        c.wait()


def mixer_body(
    at,
    docs,
    routes,
    scale,
    gain,
    bias,
    near,
    halo,
    weight,
    send,
    normed,
    own,
    weight_v,
    first_v,
    sems,
):
    y, x = at[0], at[1]
    copies = [pltpu.make_async_copy(weight.at[g], weight_v.at[g], sems.at[g]) for g in range(4)]
    for c in copies:
        c.start()
    marks = jnp.concatenate(
        [halo[16].astype(F32), as_column((docs[...] + 1).astype(F32))], axis=0
    )
    members = jnp.ones(marks.shape, F32)
    insides, counts = [], []
    for step in range(4):
        inside = jnp.where(pltpu.roll(marks, 1 << step, 0) == marks, 1.0, 0.0)
        members = members + inside * pltpu.roll(members, 1 << step, 0)
        insides.append(four(inside))
        counts.append(four(members[HALO:]))
    total = jnp.zeros((TOKENS_HERE, 1), F32)
    squares = jnp.zeros((TOKENS_HERE, 1), F32)
    for g in range(4):
        lanes = slice(g * QUARTER, (g + 1) * QUARTER)
        head = side([halo[4 * g + i] for i in range(4)]).astype(F32)
        mine = side([near[4 * g + i] for i in range(4)]).astype(F32)
        running = jnp.concatenate([head, mine], axis=0)
        for step in range(g + 1):
            running = running + insides[step] * pltpu.roll(running, 1 << step, 0)
        mixed = (running[HALO:] / counts[g] - mine).astype(BF16)
        copies[g].wait()
        projected = jnp.dot(mixed, weight_v[g], preferred_element_type=F32)
        first = RESIDUAL_SCALE * mine + projected * scale[:, lanes]
        first_v[g] = first
        part, part_squares = sums(first)
        total = total + part
        squares = squares + part_squares
    mean = total / MODEL
    inv = lax.rsqrt(squares / MODEL - mean * mean + NORM_EPS)
    for g in range(4):
        lanes = slice(g * QUARTER, (g + 1) * QUARTER)
        normed[g] = ((first_v[g] - mean) * inv * gain[:, lanes] + bias[:, lanes]).astype(BF16)
    quarter = normed[y]
    named = routes[...]
    dests = []
    for k, rank in enumerate(ranks_of(named)):
        slot = named[k : k + 1] * SLOTS_SENT + (rank >> 2)
        dests.append(jnp.where((rank & 3) == x, slot, -1))
    slot = iota((EXPERTS * SLOTS_SENT, TOKENS_HERE), 0)
    pick = chosen((slot == dests[0]) | (slot == dests[1]))
    send[...] = jnp.dot(pick, quarter, preferred_element_type=F32).astype(BF16)
    mine = quarter[:, 0:LANES]
    for i in range(1, 4):
        mine = jnp.where(x == i, quarter[:, i * LANES : (i + 1) * LANES], mine)
    own[...] = mine


def compact_body(rows, out):
    shape = (ROUTED_ROWS, EXPERTS * SLOTS_SENT)
    came = iota(shape, 1)
    within = came & 7
    goes = SLOTS_USED * (came >> 3) + within
    keep = chosen((iota(shape, 0) == goes) & (within < SLOTS_USED))
    packed = jnp.dot(keep, rows[...], preferred_element_type=F32).astype(BF16)
    for i in range(4):
        out[i] = packed


def shared_body(at, normed, s0, s1, s2, out, own_v, near_v, far_v, part_v, sems):
    copies = [
        pltpu.make_async_copy(source, target, sems.at[i])
        for i, (source, target) in enumerate(((s0, own_v), (s1, near_v), (s2, far_v)))
    ]
    for c in copies:
        c.start()
    half = pl.multiple_of((at[0] & 1) * SHARED_ROWS, SHARED_ROWS)
    shared = side([normed[i, pl.ds(half, SHARED_ROWS), :] for i in range(4)])
    for c in copies:
        c.wait()

    def units(i, lanes):
        here = slice(i * SHARED_UNITS, (i + 1) * SHARED_UNITS)
        half = slice(i * HALF_UNITS, (i + 1) * HALF_UNITS)
        return jnp.concatenate([own_v[here, lanes], near_v[half, lanes], far_v[half, lanes]], axis=0)

    contract = (((1,), (1,)), ((), ()))
    every = slice(0, MODEL)
    sg = lax.dot_general(shared, units(0, every), contract, preferred_element_type=F32)
    su = lax.dot_general(shared, units(1, every), contract, preferred_element_type=F32)
    hidden = (jax.nn.silu(sg) * su).astype(BF16)
    for b in range(0, 16, 2):
        down = units(2, slice(b * LANES, (b + 2) * LANES))
        part = jnp.dot(hidden, down, preferred_element_type=F32).astype(BF16)
        part_v[b] = part[:, :LANES]
        part_v[b + 1] = part[:, LANES:]
    send = pltpu.make_async_copy(part_v, out.at[:, pl.ds(ROUTED_ROWS, SHARED_ROWS), :], sems.at[3])
    send.start()
    send.wait()


def expert_body(rows, low, high, w0, w1, w2, w3, w4, w5, begun, out, wv, part_v, sems):
    moved = (w0, w1, w2, w3, w4, w5)
    copies = [pltpu.make_async_copy(m, wv.at[i], sems.at[i]) for i, m in enumerate(moved)]
    for c in copies:
        c.start()

    def lower(c, start, stop):
        return wv[2 * c - 2, start:stop, :] if c else low[start:stop, :]

    def upper(c, start, stop):
        start, stop = start - RELAYED, stop - RELAYED
        return wv[2 * c - 1, start:stop, :] if c else high[start:stop, :]

    tokens = side([rows[i] for i in range(4)])
    hidden = []
    for c in range(4):
        if c:
            copies[2 * c - 2].wait()
            copies[2 * c - 1].wait()
        ups = [lower(c, UP_AT, RELAYED), upper(c, RELAYED, DOWN_AT)]
        both = side([lower(c, 0, UP_AT), jnp.concatenate(ups, axis=0)])
        parts = jnp.dot(tokens, both, preferred_element_type=F32)
        hidden.append((jax.nn.silu(parts[:, :LANES]) * parts[:, LANES:]).astype(BF16))
    hidden = side(hidden)

    def block(c, b):
        return upper(c, DOWN_AT + b * LANES, DOWN_AT + (b + 1) * LANES)

    sends = []
    for b in range(0, 16, 2):
        down = jnp.concatenate([side([block(c, b), block(c, b + 1)]) for c in range(4)], axis=0)
        part = jnp.dot(hidden, down, preferred_element_type=F32).astype(BF16)
        part_v[b] = part[:, :LANES]
        part_v[b + 1] = part[:, LANES:]
        target = out.at[pl.ds(b, 2), pl.ds(0, ROUTED_ROWS), :]
        sends.append(pltpu.make_async_copy(part_v.at[pl.ds(b, 2)], target, sems.at[6 + b // 2]))
        sends[-1].start()
    for c in sends:
        c.wait()


def return_body(parts, send, shared):
    routed = []
    for x in range(4):
        total = parts[x, 0:ROUTED_ROWS, :].astype(F32)
        for y in range(1, 4):
            total = total + parts[4 * y + x, 0:ROUTED_ROWS, :].astype(F32)
        routed.append(total.astype(BF16))
    for half in range(2):
        total = jnp.zeros((SHARED_ROWS, LANES), F32)
        for y in (half, half + 2):
            for x in range(4):
                total = total + parts[4 * y + x, ROUTED_ROWS:, :].astype(F32)
        shared[half * SHARED_ROWS : (half + 1) * SHARED_ROWS, :] = total
    rows = jnp.concatenate(routed, axis=0)
    count = 4 * ROUTED_ROWS
    came = iota((1, count), 1)
    x = (
        (came >= ROUTED_ROWS).astype(jnp.int32)
        + (came >= 2 * ROUTED_ROWS).astype(jnp.int32)
        + (came >= 3 * ROUTED_ROWS).astype(jnp.int32)
    )
    within = came - ROUTED_ROWS * x
    source = (within * 10923) >> 16
    goes = 18 * source + 6 * x + within
    move = chosen(iota((count, count), 0) == goes)
    send[...] = jnp.dot(move, rows, preferred_element_type=F32).astype(BF16)


def weigh_body(routes, weight, high_out, low_out):
    named = routes[...]
    scale = weight[...]
    slot = iota((4 * ROUTED_ROWS, TOKENS_HERE), 0)
    taken = jnp.zeros(slot.shape, F32)
    for k, rank in enumerate(ranks_of(named)):
        at = named[k : k + 1] * (4 * SLOTS_USED) + SLOTS_USED * (rank & 3) + (rank >> 2)
        taken = jnp.where(slot == at, scale[k : k + 1], taken)
    taken = taken.T
    high = taken.astype(BF16)
    high_out[...] = high
    low_out[...] = (taken - high.astype(F32)).astype(BF16)


def combine_body(rows, high, low, own, shared, second_out, stats_out):
    mix = jnp.dot(high[...], rows[...], preferred_element_type=F32)
    mix = mix + jnp.dot(low[...], rows[...], preferred_element_type=F32)
    second = RESIDUAL_SCALE * own[...].astype(F32) + mix + shared[...]
    second_out[...] = second
    stats = row_stats(second)[0:2]
    for i in range(16):
        stats_out[i] = stats


def settle_body(second, stats, gain, bias, out):
    total = stats[0]
    for i in range(1, 16):
        total = total + stats[i]
    mean, inv = mean_and_scale(total)
    out[...] = ((second[...] - mean) * inv * gain[...] + bias[...]).astype(BF16)


def struct(shape, dtype):
    return pltpu.HBM(shape, dtype)


def held(shape, dtype):
    return pltpu.VMEM(shape, dtype)


def exchange(parts, axes):
    return lax.all_to_all(parts, axes, split_axis=0, concat_axis=0, tiled=True)


def around(shard, by):
    return lax.ppermute(shard, "x", [(i, (i + by) % 4) for i in range(4)])


def kernel(body, in_specs, **options):
    params = pltpu.CompilerParams(vmem_limit_bytes=24 * 1024 * 1024)
    call = pl.pallas_call(body, in_specs=in_specs, compiler_params=params, **options)
    places = {id(HELD): pltpu.VMEM, id(HBM): pltpu.HBM}

    def run(*args):
        args = [
            pltpu.with_memory_space_constraint(a, places[id(s)]) if id(s) in places else a
            for a, s in zip(args, in_specs, strict=True)
        ]
        return call(*args)

    return run


def layer(
    layer_input,
    doc_ids,
    routes,
    route_weight,
    pool_weight,
    pool_scale,
    norm1_gain,
    norm1_bias,
    expert_gate,
    expert_up,
    expert_down,
    shared_gate,
    shared_up,
    shared_down,
    norm2_gain,
    norm2_bias,
):
    core = lax.axis_index("sp") & 1
    at = jnp.stack([lax.axis_index("y"), lax.axis_index("x"), core]).astype(jnp.int32)
    spread = kernel(
        spread_body,
        out_shape=struct((16, TOKENS_HERE, LANES), BF16),
        in_specs=[HBM],
        out_specs=HBM,
        scratch_shapes=[
            pltpu.VMEM((TOKENS_HERE, LANES), BF16),
            pltpu.SemaphoreType.DMA((17,)),
        ],
    )(layer_input)
    near = exchange(spread, ("y", "x"))
    low, high, shared_packed, shared_half = kernel(
        pack_body,
        out_shape=[
            held((RELAYED, LANES), BF16),
            held((RELAYED, LANES), BF16),
            struct((3 * SHARED_UNITS, MODEL), BF16),
            struct((3 * HALF_UNITS, MODEL), BF16),
        ],
        in_specs=[SMEM] + [HBM] * 6,
        out_specs=[VMEM] * 4,
        scratch_shapes=[pltpu.SemaphoreType.DMA((25,))],
        cost_estimate=pl.CostEstimate(
            flops=10_000_000, bytes_accessed=4 * PACKED * LANES, transcendentals=0
        ),
    )(
        at,
        expert_gate[0],
        expert_up[0],
        expert_down[0],
        shared_gate.T,
        shared_up.T,
        shared_down,
    )
    marks = jnp.broadcast_to((doc_ids[-HALO:] + 1).astype(BF16)[:, None], (HALO, LANES))
    tail = jnp.concatenate([near[:, -HALO:, :], marks[None]], axis=0)
    following = [(i, i + 1) for i in range(lax.axis_size("sp") - 1)]
    halo = lax.ppermute(tail, "sp", following)
    left_low = around(low, 1)
    right_high = around(high, -1)
    left_high = around(high, 1)
    right_low = around(low, -1)
    send, normed, own = kernel(
        mixer_body,
        in_specs=[SMEM] + [VMEM] * 5 + [HELD, HELD, HBM],
        out_specs=[VMEM] * 3,
        scratch_shapes=[
            pltpu.VMEM((4, QUARTER, QUARTER), BF16),
            pltpu.VMEM((4, TOKENS_HERE, QUARTER), F32),
            pltpu.SemaphoreType.DMA((4,)),
        ],
        out_shape=[
            struct((EXPERTS * SLOTS_SENT, QUARTER), BF16),
            held((4, TOKENS_HERE, QUARTER), BF16),
            held((TOKENS_HERE, LANES), BF16),
        ],
    )(
        at,
        doc_ids[None],
        routes.T,
        pool_scale[None],
        norm1_gain[None],
        norm1_bias[None],
        near,
        halo,
        pool_weight,
    )
    from_pair = lax.ppermute(shared_half, "y", [(i, i ^ 1) for i in range(4)])
    cores = [(i, i ^ 1) for i in range(lax.axis_size("sp"))]
    from_core = lax.ppermute(from_pair, "sp", cores)
    across_low = around(left_low, 1)
    across_high = around(right_high, -1)
    arrived = exchange(send.reshape(EXPERTS, SLOTS_SENT, QUARTER), "sp")
    gather_in = kernel(
        compact_body,
        out_shape=struct((4, ROUTED_ROWS, QUARTER), BF16),
        in_specs=[HELD],
        out_specs=VMEM,
    )(arrived.reshape(EXPERTS * SLOTS_SENT, QUARTER))
    gathered = exchange(gather_in, "y")
    begun = kernel(
        shared_body,
        out_shape=struct((16, ROUTED_ROWS + SHARED_ROWS, LANES), BF16),
        in_specs=[SMEM, HELD, HBM, HBM, ANY],
        out_specs=HBM,
        scratch_shapes=[
            pltpu.VMEM((3 * SHARED_UNITS, MODEL), BF16),
            pltpu.VMEM((3 * HALF_UNITS, MODEL), BF16),
            pltpu.VMEM((3 * HALF_UNITS, MODEL), BF16),
            pltpu.VMEM((16, SHARED_ROWS, LANES), BF16),
            pltpu.SemaphoreType.DMA((4,)),
        ],
    )(at, normed, shared_packed, from_pair, from_core)
    partial = kernel(
        expert_body,
        out_shape=struct((16, ROUTED_ROWS + SHARED_ROWS, LANES), BF16),
        in_specs=[HELD] * 3 + [HBM] * 7,
        out_specs=HBM,
        scratch_shapes=[
            pltpu.VMEM((6, RELAYED, LANES), BF16),
            pltpu.VMEM((16, ROUTED_ROWS, LANES), BF16),
            pltpu.SemaphoreType.DMA((14,)),
        ],
        input_output_aliases={9: 0},
    )(
        gathered,
        low,
        high,
        left_low,
        left_high,
        right_low,
        right_high,
        across_low,
        across_high,
        begun,
    )
    parts = exchange(partial, ("y", "x"))
    back, shared_sum = kernel(
        return_body,
        out_shape=[
            struct((4 * ROUTED_ROWS, LANES), BF16),
            held((TOKENS_HERE, LANES), F32),
        ],
        in_specs=[HELD],
        out_specs=[VMEM, VMEM],
    )(parts)
    returned = exchange(back.reshape(EXPERTS, 4 * SLOTS_USED, LANES), "sp")
    high_weights, low_weights = kernel(
        weigh_body,
        out_shape=[held((TOKENS_HERE, 4 * ROUTED_ROWS), BF16)] * 2,
        in_specs=[VMEM] * 2,
        out_specs=[VMEM] * 2,
    )(routes.T, route_weight.T)
    second, row_sums = kernel(
        combine_body,
        out_shape=[held((TOKENS_HERE, LANES), F32), struct((16, 2, TOKENS_HERE), F32)],
        in_specs=[HELD] * 5,
        out_specs=[VMEM, VMEM],
    )(returned.reshape(4 * ROUTED_ROWS, LANES), high_weights, low_weights, own, shared_sum)
    row_sums = exchange(row_sums, ("y", "x"))
    return kernel(
        settle_body,
        out_shape=jax.ShapeDtypeStruct((TOKENS_HERE, LANES), BF16),
        in_specs=[HELD, HELD, VMEM, VMEM],
        out_specs=VMEM,
    )(second, row_sums, norm2_gain[None], norm2_bias[None])


def solution(mesh):
    split = Mesh(mesh.devices.reshape(mesh.shape["sp"], 4, 4), ("sp", "y", "x"))
    tp = ("y", "x")
    placed = (
        P("sp", tp),
        P("sp"),
        P("sp", None),
        P("sp", None),
        P(),
        P(),
        P(),
        P(),
        P("sp", None, tp),
        P("sp", None, tp),
        P("sp", tp, None),
        P(None, tp),
        P(None, tp),
        P(tp, None),
        P(tp),
        P(tp),
    )
    return jax.shard_map(layer, mesh=split, in_specs=placed, out_specs=P("sp", tp), check_vma=False)
```

```python
import jax
import jax.numpy as jnp
from jax import lax
from jax.experimental import pallas as pl
from jax.experimental.pallas import tpu as pltpu
from jax.sharding import Mesh
from jax.sharding import PartitionSpec as P


RESIDUAL_SCALE = 2.0**0.5
NORM_EPS = 1e-05
HALO = 16
F32 = jnp.float32
BF16 = jnp.bfloat16
VMEM = pl.BlockSpec(memory_space=pltpu.VMEM)
HELD = pl.BlockSpec(memory_space=pltpu.VMEM)
HBM = pl.BlockSpec(memory_space=pltpu.HBM)
ANY = pl.BlockSpec(memory_space=pl.ANY)
SMEM = pl.BlockSpec(memory_space=pltpu.SMEM)

TOKENS_HERE = 256
EXPERTS = 32
LANES = 128
QUARTER = 512
MODEL = 2048
SLOTS_SENT = 8
SLOTS_USED = 6
ROUTED_ROWS = EXPERTS * SLOTS_USED
SHARED_ROWS = 128
UP_AT = 2048
DOWN_AT = 4096
PACKED = 6144
SHARED_UNITS = 64
HALF_UNITS = SHARED_UNITS // 2
RELAYED = PACKED // 2


def iota(shape, dim):
    return lax.broadcasted_iota(jnp.int32, shape, dim)


def side(parts):
    return jnp.concatenate(parts, axis=1)


def four(a):
    return jnp.concatenate([a, a, a, a], axis=1)


def as_column(row):
    return jnp.broadcast_to(row, (LANES, row.shape[1])).T


def chosen(mask):
    return mask.astype(F32).astype(BF16)


def sums(values):
    total = jnp.sum(values, axis=1, keepdims=True)
    return total, jnp.sum(values * values, axis=1, keepdims=True)


def row_stats(values):
    lane = iota((values.shape[0], LANES), 1)
    total, squares = sums(values)
    return jnp.where(lane == 0, total, jnp.where(lane == 1, squares, 0.0)).T


def mean_and_scale(total):
    mean = total[0:1] / MODEL
    var = total[1:2] / MODEL - mean * mean
    return as_column(mean), as_column(lax.rsqrt(var + NORM_EPS))


def ranks_of(routes):
    expert = iota((EXPERTS, TOKENS_HERE), 0)
    picks = [routes[k : k + 1] == expert for k in range(2)]
    named = chosen(picks[0] | picks[1])
    earlier = chosen(iota((TOKENS_HERE, TOKENS_HERE), 0) < iota((TOKENS_HERE, TOKENS_HERE), 1))
    counts = jnp.dot(named, earlier, preferred_element_type=F32)
    return [
        jnp.sum(jnp.where(p, counts, 0.0), axis=0, keepdims=True).astype(jnp.int32) for p in picks
    ]


def pack_body(at, gate, up, down, sgate, sup, sdown, low, high, shared_out, half_out, sems):
    core = pl.multiple_of(at[2] * HALF_UNITS, HALF_UNITS)
    rest = DOWN_AT - RELAYED
    plan = [
        (gate, low.at[pl.ds(0, UP_AT)]),
        (up.at[pl.ds(0, RELAYED - UP_AT)], low.at[pl.ds(UP_AT, RELAYED - UP_AT)]),
        (up.at[pl.ds(RELAYED - UP_AT, rest)], high.at[pl.ds(0, rest)]),
    ]
    for b in range(16):
        lanes = pl.ds(b * LANES, LANES)
        plan.append((down.at[:, lanes], high.at[pl.ds(rest + b * LANES, LANES)]))
    for i, part in enumerate((sgate, sup, sdown)):
        plan.append((part, shared_out.at[pl.ds(i * SHARED_UNITS, SHARED_UNITS)]))
        mine = part.at[pl.ds(core, HALF_UNITS)]
        plan.append((mine, half_out.at[pl.ds(i * HALF_UNITS, HALF_UNITS)]))
    copies = [pltpu.make_async_copy(s, d, sems.at[i]) for i, (s, d) in enumerate(plan)]
    for c in copies:
        c.start()
    for c in copies:
        c.wait()


def spread_body(shard, out, block, sems):
    move = pltpu.make_async_copy(shard, block, sems.at[16])
    move.start()
    move.wait()
    copies = [pltpu.make_async_copy(block, out.at[i], sems.at[i]) for i in range(16)]
    for c in copies:
        c.start()
    for c in copies:
        c.wait()


def mixer_body(
    at,
    docs,
    routes,
    scale,
    gain,
    bias,
    near,
    halo,
    weight,
    send,
    normed,
    own,
    weight_v,
    mixed_v,
    first_v,
    sems,
):
    y, x = at[0], at[1]
    copies = [pltpu.make_async_copy(weight.at[g], weight_v.at[g], sems.at[g]) for g in range(4)]
    for c in copies:
        c.start()
    marks = jnp.concatenate(
        [halo[16].astype(F32), as_column((docs[...] + 1).astype(F32))], axis=0
    )
    members = jnp.ones(marks.shape, F32)
    insides, counts = [], []
    for step in range(4):
        inside = jnp.where(pltpu.roll(marks, 1 << step, 0) == marks, 1.0, 0.0)
        members = members + inside * pltpu.roll(members, 1 << step, 0)
        insides.append(four(inside))
        counts.append(four(1.0 / members[HALO:]))
    for g in range(4):
        head = side([halo[4 * g + i] for i in range(4)]).astype(F32)
        mine = side([near[4 * g + i] for i in range(4)]).astype(F32)
        running = jnp.concatenate([head, mine], axis=0)
        for step in range(g + 1):
            running = running + insides[step] * pltpu.roll(running, 1 << step, 0)
        mixed_v[g] = (running[HALO:] * counts[g] - mine).astype(BF16)
    total = jnp.zeros((TOKENS_HERE, 1), F32)
    squares = jnp.zeros((TOKENS_HERE, 1), F32)
    for g in range(4):
        lanes = slice(g * QUARTER, (g + 1) * QUARTER)
        copies[g].wait()
        projected = jnp.dot(mixed_v[g], weight_v[g], preferred_element_type=F32)
        mine = side([near[4 * g + i] for i in range(4)]).astype(F32)
        first = RESIDUAL_SCALE * mine + projected * scale[:, lanes]
        first_v[g] = first
        part, part_squares = sums(first)
        total = total + part
        squares = squares + part_squares
    mean = total / MODEL
    inv = lax.rsqrt(squares / MODEL - mean * mean + NORM_EPS)
    for g in range(4):
        lanes = slice(g * QUARTER, (g + 1) * QUARTER)
        normed[g] = ((first_v[g] - mean) * inv * gain[:, lanes] + bias[:, lanes]).astype(BF16)
    quarter = normed[y]
    named = routes[...]
    dests = []
    for k, rank in enumerate(ranks_of(named)):
        slot = named[k : k + 1] * SLOTS_SENT + (rank >> 2)
        dests.append(jnp.where((rank & 3) == x, slot, -1))
    slot = iota((EXPERTS * SLOTS_SENT, TOKENS_HERE), 0)
    pick = chosen((slot == dests[0]) | (slot == dests[1]))
    send[...] = jnp.dot(pick, quarter, preferred_element_type=F32).astype(BF16)
    mine = quarter[:, 0:LANES]
    for i in range(1, 4):
        mine = jnp.where(x == i, quarter[:, i * LANES : (i + 1) * LANES], mine)
    own[...] = mine


def compact_body(rows, out):
    shape = (ROUTED_ROWS, EXPERTS * SLOTS_SENT)
    came = iota(shape, 1)
    within = came & 7
    goes = SLOTS_USED * (came >> 3) + within
    keep = chosen((iota(shape, 0) == goes) & (within < SLOTS_USED))
    packed = jnp.dot(keep, rows[...], preferred_element_type=F32).astype(BF16)
    for i in range(4):
        out[i] = packed


def shared_body(at, normed, s0, s1, s2, out, own_v, near_v, far_v, part_v, sems):
    copies = [
        pltpu.make_async_copy(source, target, sems.at[i])
        for i, (source, target) in enumerate(((s0, own_v), (s1, near_v), (s2, far_v)))
    ]
    for c in copies:
        c.start()
    half = pl.multiple_of((at[0] & 1) * SHARED_ROWS, SHARED_ROWS)
    shared = side([normed[i, pl.ds(half, SHARED_ROWS), :] for i in range(4)])
    for c in copies:
        c.wait()

    def units(i, lanes):
        here = slice(i * SHARED_UNITS, (i + 1) * SHARED_UNITS)
        half = slice(i * HALF_UNITS, (i + 1) * HALF_UNITS)
        return jnp.concatenate([own_v[here, lanes], near_v[half, lanes], far_v[half, lanes]], axis=0)

    contract = (((1,), (1,)), ((), ()))
    every = slice(0, MODEL)
    sg = lax.dot_general(shared, units(0, every), contract, preferred_element_type=F32)
    su = lax.dot_general(shared, units(1, every), contract, preferred_element_type=F32)
    hidden = (jax.nn.silu(sg) * su).astype(BF16)
    for b in range(0, 16, 2):
        down = units(2, slice(b * LANES, (b + 2) * LANES))
        part = jnp.dot(hidden, down, preferred_element_type=F32).astype(BF16)
        part_v[b] = part[:, :LANES]
        part_v[b + 1] = part[:, LANES:]
    send = pltpu.make_async_copy(part_v, out.at[:, pl.ds(ROUTED_ROWS, SHARED_ROWS), :], sems.at[3])
    send.start()
    send.wait()


def expert_body(rows, w0, w1, w2, w3, w4, w5, w6, w7, begun, out, wv, part_v, sems):
    moved = (w1, w2, w3, w4, w5, w6, w7)
    copies = [pltpu.make_async_copy(m, wv.at[i], sems.at[i]) for i, m in enumerate(moved)]
    for c in copies:
        c.start()
    shards = (w0,) + tuple(wv.at[i] for i in range(7))

    def lower(c, start, stop):
        return shards[2 * c][start:stop, :]

    def upper(c, start, stop):
        return shards[2 * c + 1][start - RELAYED : stop - RELAYED, :]

    tokens = side([rows[i] for i in range(4)])
    hidden = []
    for c in range(4):
        for i in ((0,), (1, 2), (3, 4), (5, 6))[c]:
            copies[i].wait()
        ups = [lower(c, UP_AT, RELAYED), upper(c, RELAYED, DOWN_AT)]
        both = side([lower(c, 0, UP_AT), jnp.concatenate(ups, axis=0)])
        parts = jnp.dot(tokens, both, preferred_element_type=F32)
        hidden.append((jax.nn.silu(parts[:, :LANES]) * parts[:, LANES:]).astype(BF16))
    hidden = side(hidden)

    def block(c, b):
        return upper(c, DOWN_AT + b * LANES, DOWN_AT + (b + 1) * LANES)

    sends = []
    for b in range(0, 16, 2):
        down = jnp.concatenate([side([block(c, b), block(c, b + 1)]) for c in range(4)], axis=0)
        part = jnp.dot(hidden, down, preferred_element_type=F32).astype(BF16)
        part_v[b] = part[:, :LANES]
        part_v[b + 1] = part[:, LANES:]
        target = out.at[pl.ds(b, 2), pl.ds(0, ROUTED_ROWS), :]
        sends.append(pltpu.make_async_copy(part_v.at[pl.ds(b, 2)], target, sems.at[7 + b // 2]))
        sends[-1].start()
    for c in sends:
        c.wait()


def return_body(parts, send, shared):
    routed = []
    for x in range(4):
        total = parts[x, 0:ROUTED_ROWS, :].astype(F32)
        for y in range(1, 4):
            total = total + parts[4 * y + x, 0:ROUTED_ROWS, :].astype(F32)
        routed.append(total.astype(BF16))
    for half in range(2):
        total = jnp.zeros((SHARED_ROWS, LANES), F32)
        for y in (half, half + 2):
            for x in range(4):
                total = total + parts[4 * y + x, ROUTED_ROWS:, :].astype(F32)
        shared[half * SHARED_ROWS : (half + 1) * SHARED_ROWS, :] = total
    rows = jnp.concatenate(routed, axis=0)
    count = 4 * ROUTED_ROWS
    came = iota((1, count), 1)
    x = (
        (came >= ROUTED_ROWS).astype(jnp.int32)
        + (came >= 2 * ROUTED_ROWS).astype(jnp.int32)
        + (came >= 3 * ROUTED_ROWS).astype(jnp.int32)
    )
    within = came - ROUTED_ROWS * x
    source = (within * 10923) >> 16
    goes = 18 * source + 6 * x + within
    move = chosen(iota((count, count), 0) == goes)
    send[...] = jnp.dot(move, rows, preferred_element_type=F32).astype(BF16)


def weigh_body(routes, weight, high_out, low_out):
    named = routes[...]
    scale = weight[...]
    slot = iota((4 * ROUTED_ROWS, TOKENS_HERE), 0)
    taken = jnp.zeros(slot.shape, F32)
    for k, rank in enumerate(ranks_of(named)):
        at = named[k : k + 1] * (4 * SLOTS_USED) + SLOTS_USED * (rank & 3) + (rank >> 2)
        taken = jnp.where(slot == at, scale[k : k + 1], taken)
    taken = taken.T
    high = taken.astype(BF16)
    high_out[...] = high
    low_out[...] = (taken - high.astype(F32)).astype(BF16)


def combine_body(rows, high, low, own, shared, second_out, stats_out):
    mix = jnp.dot(high[...], rows[...], preferred_element_type=F32)
    mix = mix + jnp.dot(low[...], rows[...], preferred_element_type=F32)
    second = RESIDUAL_SCALE * own[...].astype(F32) + mix + shared[...]
    second_out[...] = second
    stats = row_stats(second)[0:2]
    for i in range(16):
        stats_out[i] = stats


def settle_body(second, stats, gain, bias, out):
    total = stats[0]
    for i in range(1, 16):
        total = total + stats[i]
    mean, inv = mean_and_scale(total)
    out[...] = ((second[...] - mean) * inv * gain[...] + bias[...]).astype(BF16)


def struct(shape, dtype):
    return pltpu.HBM(shape, dtype)


def held(shape, dtype):
    return pltpu.VMEM(shape, dtype)


def exchange(parts, axes):
    return lax.all_to_all(parts, axes, split_axis=0, concat_axis=0, tiled=True)


def around(shard, by):
    return lax.ppermute(shard, "x", [(i, (i + by) % 4) for i in range(4)])


def kernel(body, in_specs, **options):
    params = pltpu.CompilerParams(vmem_limit_bytes=24 * 1024 * 1024)
    call = pl.pallas_call(body, in_specs=in_specs, compiler_params=params, **options)
    places = {id(HELD): pltpu.VMEM, id(HBM): pltpu.HBM}

    def run(*args):
        args = [
            pltpu.with_memory_space_constraint(a, places[id(s)]) if id(s) in places else a
            for a, s in zip(args, in_specs, strict=True)
        ]
        return call(*args)

    return run


def layer(
    layer_input,
    doc_ids,
    routes,
    route_weight,
    pool_weight,
    pool_scale,
    norm1_gain,
    norm1_bias,
    expert_gate,
    expert_up,
    expert_down,
    shared_gate,
    shared_up,
    shared_down,
    norm2_gain,
    norm2_bias,
):
    core = lax.axis_index("sp") & 1
    at = jnp.stack([lax.axis_index("y"), lax.axis_index("x"), core]).astype(jnp.int32)
    spread = kernel(
        spread_body,
        out_shape=struct((16, TOKENS_HERE, LANES), BF16),
        in_specs=[HBM],
        out_specs=HBM,
        scratch_shapes=[
            pltpu.VMEM((TOKENS_HERE, LANES), BF16),
            pltpu.SemaphoreType.DMA((17,)),
        ],
    )(layer_input)
    near = exchange(spread, ("y", "x"))
    low, high, shared_packed, shared_half = kernel(
        pack_body,
        out_shape=[
            held((RELAYED, LANES), BF16),
            held((RELAYED, LANES), BF16),
            struct((3 * SHARED_UNITS, MODEL), BF16),
            struct((3 * HALF_UNITS, MODEL), BF16),
        ],
        in_specs=[SMEM] + [HBM] * 6,
        out_specs=[VMEM] * 4,
        scratch_shapes=[pltpu.SemaphoreType.DMA((25,))],
        cost_estimate=pl.CostEstimate(
            flops=10_000_000, bytes_accessed=4 * PACKED * LANES, transcendentals=0
        ),
    )(
        at,
        expert_gate[0],
        expert_up[0],
        expert_down[0],
        shared_gate.T,
        shared_up.T,
        shared_down,
    )
    marks = jnp.broadcast_to((doc_ids[-HALO:] + 1).astype(BF16)[:, None], (HALO, LANES))
    tail = jnp.concatenate([near[:, -HALO:, :], marks[None]], axis=0)
    following = [(i, i + 1) for i in range(lax.axis_size("sp") - 1)]
    halo = lax.ppermute(tail, "sp", following)
    left_low = around(low, 1)
    right_high = around(high, -1)
    left_high = around(high, 1)
    right_low = around(low, -1)
    send, normed, own = kernel(
        mixer_body,
        in_specs=[SMEM] + [VMEM] * 5 + [HELD, HELD, HBM],
        out_specs=[VMEM] * 3,
        scratch_shapes=[
            pltpu.VMEM((4, QUARTER, QUARTER), BF16),
            pltpu.VMEM((4, TOKENS_HERE, QUARTER), BF16),
            pltpu.VMEM((4, TOKENS_HERE, QUARTER), F32),
            pltpu.SemaphoreType.DMA((4,)),
        ],
        out_shape=[
            struct((EXPERTS * SLOTS_SENT, QUARTER), BF16),
            held((4, TOKENS_HERE, QUARTER), BF16),
            held((TOKENS_HERE, LANES), BF16),
        ],
    )(
        at,
        doc_ids[None],
        routes.T,
        pool_scale[None],
        norm1_gain[None],
        norm1_bias[None],
        near,
        halo,
        pool_weight,
    )
    from_pair = lax.ppermute(shared_half, "y", [(i, i ^ 1) for i in range(4)])
    cores = [(i, i ^ 1) for i in range(lax.axis_size("sp"))]
    from_core = lax.ppermute(from_pair, "sp", cores)
    across_low = around(left_low, 1)
    across_high = around(right_high, -1)
    arrived = exchange(send.reshape(EXPERTS, SLOTS_SENT, QUARTER), "sp")
    gather_in = kernel(
        compact_body,
        out_shape=struct((4, ROUTED_ROWS, QUARTER), BF16),
        in_specs=[HELD],
        out_specs=VMEM,
    )(arrived.reshape(EXPERTS * SLOTS_SENT, QUARTER))
    gathered = exchange(gather_in, "y")
    begun = kernel(
        shared_body,
        out_shape=struct((16, ROUTED_ROWS + SHARED_ROWS, LANES), BF16),
        in_specs=[SMEM, HELD, HBM, HBM, ANY],
        out_specs=HBM,
        scratch_shapes=[
            pltpu.VMEM((3 * SHARED_UNITS, MODEL), BF16),
            pltpu.VMEM((3 * HALF_UNITS, MODEL), BF16),
            pltpu.VMEM((3 * HALF_UNITS, MODEL), BF16),
            pltpu.VMEM((16, SHARED_ROWS, LANES), BF16),
            pltpu.SemaphoreType.DMA((4,)),
        ],
    )(at, normed, shared_packed, from_pair, from_core)
    partial = kernel(
        expert_body,
        out_shape=struct((16, ROUTED_ROWS + SHARED_ROWS, LANES), BF16),
        in_specs=[HELD] * 2 + [HBM] * 8,
        out_specs=HBM,
        scratch_shapes=[
            pltpu.VMEM((7, RELAYED, LANES), BF16),
            pltpu.VMEM((16, ROUTED_ROWS, LANES), BF16),
            pltpu.SemaphoreType.DMA((15,)),
        ],
        input_output_aliases={9: 0},
    )(
        gathered,
        low,
        high,
        left_low,
        left_high,
        right_low,
        right_high,
        across_low,
        across_high,
        begun,
    )
    parts = exchange(partial, ("y", "x"))
    back, shared_sum = kernel(
        return_body,
        out_shape=[
            struct((4 * ROUTED_ROWS, LANES), BF16),
            held((TOKENS_HERE, LANES), F32),
        ],
        in_specs=[HELD],
        out_specs=[VMEM, VMEM],
    )(parts)
    returned = exchange(back.reshape(EXPERTS, 4 * SLOTS_USED, LANES), "sp")
    high_weights, low_weights = kernel(
        weigh_body,
        out_shape=[held((TOKENS_HERE, 4 * ROUTED_ROWS), BF16)] * 2,
        in_specs=[VMEM] * 2,
        out_specs=[VMEM] * 2,
    )(routes.T, route_weight.T)
    second, row_sums = kernel(
        combine_body,
        out_shape=[held((TOKENS_HERE, LANES), F32), struct((16, 2, TOKENS_HERE), F32)],
        in_specs=[HELD] * 5,
        out_specs=[VMEM, VMEM],
    )(returned.reshape(4 * ROUTED_ROWS, LANES), high_weights, low_weights, own, shared_sum)
    row_sums = exchange(row_sums, ("y", "x"))
    return kernel(
        settle_body,
        out_shape=jax.ShapeDtypeStruct((TOKENS_HERE, LANES), BF16),
        in_specs=[HELD, HELD, VMEM, VMEM],
        out_specs=VMEM,
    )(second, row_sums, norm2_gain[None], norm2_bias[None])


def solution(mesh):
    split = Mesh(mesh.devices.reshape(mesh.shape["sp"], 4, 4), ("sp", "y", "x"))
    tp = ("y", "x")
    placed = (
        P("sp", tp),
        P("sp"),
        P("sp", None),
        P("sp", None),
        P(),
        P(),
        P(),
        P(),
        P("sp", None, tp),
        P("sp", None, tp),
        P("sp", tp, None),
        P(None, tp),
        P(None, tp),
        P(tp, None),
        P(tp),
        P(tp),
    )
    return jax.shard_map(layer, mesh=split, in_specs=placed, out_specs=P("sp", tp), check_vma=False)
```

```python
import jax
import jax.numpy as jnp
from jax import lax
from jax.experimental import pallas as pl
from jax.experimental.pallas import tpu as pltpu
from jax.sharding import Mesh
from jax.sharding import PartitionSpec as P


RESIDUAL_SCALE = 2.0**0.5
NORM_EPS = 1e-05
HALO = 16
F32 = jnp.float32
BF16 = jnp.bfloat16
VMEM = pl.BlockSpec(memory_space=pltpu.VMEM)
HELD = pl.BlockSpec(memory_space=pltpu.VMEM)
HBM = pl.BlockSpec(memory_space=pltpu.HBM)
ANY = pl.BlockSpec(memory_space=pl.ANY)
SMEM = pl.BlockSpec(memory_space=pltpu.SMEM)

TOKENS_HERE = 256
EXPERTS = 32
LANES = 128
QUARTER = 512
MODEL = 2048
SLOTS_SENT = 8
SLOTS_USED = 6
ROUTED_ROWS = EXPERTS * SLOTS_USED
SHARED_ROWS = 128
UP_AT = 2048
DOWN_AT = 4096
PACKED = 6144
SHARED_UNITS = 64
HALF_UNITS = SHARED_UNITS // 2
RELAYED = PACKED // 2


def iota(shape, dim):
    return lax.broadcasted_iota(jnp.int32, shape, dim)


def side(parts):
    return jnp.concatenate(parts, axis=1)


def as_column(row):
    return jnp.broadcast_to(row, (LANES, row.shape[1])).T


def chosen(mask):
    return mask.astype(F32).astype(BF16)


def sums(values):
    total = jnp.sum(values, axis=1, keepdims=True)
    return total, jnp.sum(values * values, axis=1, keepdims=True)


def row_stats(values):
    lane = iota((values.shape[0], LANES), 1)
    total, squares = sums(values)
    return jnp.where(lane == 0, total, jnp.where(lane == 1, squares, 0.0)).T


def mean_and_scale(total):
    mean = total[0:1] / MODEL
    var = total[1:2] / MODEL - mean * mean
    return as_column(mean), as_column(lax.rsqrt(var + NORM_EPS))


def ranks_of(routes):
    expert = iota((EXPERTS, TOKENS_HERE), 0)
    picks = [routes[k : k + 1] == expert for k in range(2)]
    named = chosen(picks[0] | picks[1])
    earlier = chosen(iota((TOKENS_HERE, TOKENS_HERE), 0) < iota((TOKENS_HERE, TOKENS_HERE), 1))
    counts = jnp.dot(named, earlier, preferred_element_type=F32)
    return [
        jnp.sum(jnp.where(p, counts, 0.0), axis=0, keepdims=True).astype(jnp.int32) for p in picks
    ]


def pack_body(at, gate, up, down, sgate, sup, sdown, low, high, shared_out, half_out, sems):
    core = pl.multiple_of(at[2] * HALF_UNITS, HALF_UNITS)
    rest = DOWN_AT - RELAYED
    plan = [
        (gate, low.at[pl.ds(0, UP_AT)]),
        (up.at[pl.ds(0, RELAYED - UP_AT)], low.at[pl.ds(UP_AT, RELAYED - UP_AT)]),
        (up.at[pl.ds(RELAYED - UP_AT, rest)], high.at[pl.ds(0, rest)]),
    ]
    for b in range(16):
        lanes = pl.ds(b * LANES, LANES)
        plan.append((down.at[:, lanes], high.at[pl.ds(rest + b * LANES, LANES)]))
    for i, part in enumerate((sgate, sup, sdown)):
        plan.append((part, shared_out.at[pl.ds(i * SHARED_UNITS, SHARED_UNITS)]))
        mine = part.at[pl.ds(core, HALF_UNITS)]
        plan.append((mine, half_out.at[pl.ds(i * HALF_UNITS, HALF_UNITS)]))
    copies = [pltpu.make_async_copy(s, d, sems.at[i]) for i, (s, d) in enumerate(plan)]
    for c in copies:
        c.start()
    for c in copies:
        c.wait()


def spread_body(shard, out, block, sems):
    move = pltpu.make_async_copy(shard, block, sems.at[16])
    move.start()
    move.wait()
    copies = [pltpu.make_async_copy(block, out.at[i], sems.at[i]) for i in range(16)]
    for c in copies:
        c.start()
    for c in copies:
        c.wait()


def mixer_body(
    at,
    docs,
    routes,
    scale,
    gain,
    bias,
    near,
    halo,
    weight,
    send,
    normed,
    own,
    weight_v,
    mixed_v,
    first_v,
    quarter_v,
    send_v,
    sems,
):
    y, x = at[0], at[1]
    copies = [pltpu.make_async_copy(weight.at[g], weight_v.at[g], sems.at[g]) for g in range(4)]
    for c in copies:
        c.start()
    own_row = (docs[...] + 1).astype(F32)
    own_marks = as_column(own_row)
    halo_row = halo[16].astype(F32).T[0:1]
    apart = iota((TOKENS_HERE, TOKENS_HERE), 0) - iota((TOKENS_HERE, TOKENS_HERE), 1)
    inside = (side([own_marks, own_marks]) == own_row) & (apart >= 0)
    corner = iota((HALO, HALO), 0) - iota((HALO, HALO), 1) + HALO
    corner_inside = own_marks[0:HALO, 0:HALO] == halo_row
    for g in range(4):
        window = 2 << g
        band = jnp.where(inside & (apart < window), 1.0, 0.0)
        edge = jnp.where(corner_inside & (corner < window), 1.0, 0.0)
        members = jnp.sum(band, axis=1, keepdims=True)
        first_members = members[0:HALO] + jnp.sum(edge, axis=1, keepdims=True)
        scale_by = 1.0 / jnp.concatenate([first_members, members[HALO:]], axis=0)
        band, edge = band.astype(BF16), edge.astype(BF16)
        for j in range(2):
            at_lane = slice(j * 2 * LANES, (j + 1) * 2 * LANES)
            mine = side([near[4 * g + 2 * j], near[4 * g + 2 * j + 1]])
            head = side([halo[4 * g + 2 * j], halo[4 * g + 2 * j + 1]])
            running = jnp.dot(band, mine, preferred_element_type=F32)
            begin = running[0:HALO] + jnp.dot(edge, head, preferred_element_type=F32)
            running = jnp.concatenate([begin, running[HALO:]], axis=0)
            mixed_v[g, :, at_lane] = (running * scale_by - mine.astype(F32)).astype(BF16)
    total = jnp.zeros((TOKENS_HERE, 1), F32)
    squares = jnp.zeros((TOKENS_HERE, 1), F32)
    for g in range(4):
        copies[g].wait()
        for j in range(2):
            at_lane = slice(j * 2 * LANES, (j + 1) * 2 * LANES)
            lanes = slice(g * QUARTER + j * 2 * LANES, g * QUARTER + (j + 1) * 2 * LANES)
            projected = jnp.dot(mixed_v[g], weight_v[g, :, at_lane], preferred_element_type=F32)
            mine = side([near[4 * g + 2 * j], near[4 * g + 2 * j + 1]]).astype(F32)
            first = RESIDUAL_SCALE * mine + projected * scale[:, lanes]
            first_v[g, :, at_lane] = first
            part, part_squares = sums(first)
            total = total + part
            squares = squares + part_squares
    mean = total / MODEL
    inv = lax.rsqrt(squares / MODEL - mean * mean + NORM_EPS)
    lanes = pl.ds(pl.multiple_of(y * QUARTER, QUARTER), QUARTER)
    gain_here, bias_here = gain[:, lanes], bias[:, lanes]
    for r in range(0, TOKENS_HERE, 64):
        rows = slice(r, r + 64)
        scaled = (first_v[y, rows, :] - mean[rows]) * inv[rows]
        quarter_v[rows, :] = (scaled * gain_here + bias_here).astype(BF16)
    quarter = quarter_v[...]
    named = routes[...]
    dests = []
    for k, rank in enumerate(ranks_of(named)):
        slot = named[k : k + 1] * SLOTS_SENT + (rank >> 2)
        dests.append(jnp.where((rank & 3) == x, slot, -1))
    slot = iota((EXPERTS * SLOTS_SENT, TOKENS_HERE), 0)
    pick = chosen((slot == dests[0]) | (slot == dests[1]))
    send_v[...] = jnp.dot(pick, quarter, preferred_element_type=F32).astype(BF16)
    leave = pltpu.make_async_copy(send_v, send, sems.at[4])
    leave.start()
    mine = quarter[:, 0:LANES]
    for i in range(1, 4):
        mine = jnp.where(x == i, quarter[:, i * LANES : (i + 1) * LANES], mine)
    own[...] = mine
    upper = (y & 1) == 1
    half = pl.multiple_of((y & 1) * SHARED_ROWS, SHARED_ROWS)
    mean = jnp.where(upper, mean[SHARED_ROWS:], mean[:SHARED_ROWS])
    inv = jnp.where(upper, inv[SHARED_ROWS:], inv[:SHARED_ROWS])
    for r in range(0, SHARED_ROWS, 64):
        rows = slice(r, r + 64)
        for g in range(4):
            lanes = slice(g * QUARTER, (g + 1) * QUARTER)
            scaled = (first_v[g, pl.ds(half + r, 64), :] - mean[rows]) * inv[rows]
            normed[g, rows, :] = (scaled * gain[:, lanes] + bias[:, lanes]).astype(BF16)
    leave.wait()


def compact_body(rows, out):
    shape = (ROUTED_ROWS, EXPERTS * SLOTS_SENT)
    came = iota(shape, 1)
    within = came & 7
    goes = SLOTS_USED * (came >> 3) + within
    keep = chosen((iota(shape, 0) == goes) & (within < SLOTS_USED))
    packed = jnp.dot(keep, rows[...], preferred_element_type=F32).astype(BF16)
    for i in range(4):
        out[i] = packed


def shared_body(normed, s0, s1, s2, out, own_v, near_v, far_v, part_v, sems):
    copies = [
        pltpu.make_async_copy(source, target, sems.at[i])
        for i, (source, target) in enumerate(((s0, own_v), (s1, near_v), (s2, far_v)))
    ]
    for c in copies:
        c.start()
    shared = side([normed[i] for i in range(4)])
    for c in copies:
        c.wait()

    def units(i, lanes):
        here = slice(i * SHARED_UNITS, (i + 1) * SHARED_UNITS)
        half = slice(i * HALF_UNITS, (i + 1) * HALF_UNITS)
        return jnp.concatenate([own_v[here, lanes], near_v[half, lanes], far_v[half, lanes]], axis=0)

    contract = (((1,), (1,)), ((), ()))
    every = slice(0, MODEL)
    sg = lax.dot_general(shared, units(0, every), contract, preferred_element_type=F32)
    su = lax.dot_general(shared, units(1, every), contract, preferred_element_type=F32)
    hidden = (jax.nn.silu(sg) * su).astype(BF16)
    for b in range(0, 16, 2):
        down = units(2, slice(b * LANES, (b + 2) * LANES))
        part = jnp.dot(hidden, down, preferred_element_type=F32).astype(BF16)
        part_v[b] = part[:, :LANES]
        part_v[b + 1] = part[:, LANES:]
    send = pltpu.make_async_copy(part_v, out.at[:, pl.ds(ROUTED_ROWS, SHARED_ROWS), :], sems.at[3])
    send.start()
    send.wait()


def expert_body(rows, w0, w1, w2, w3, w4, w5, w6, w7, begun, out, wv, part_v, sems):
    moved = (w1, w2, w3, w4, w5, w6, w7)
    copies = [pltpu.make_async_copy(m, wv.at[i], sems.at[i]) for i, m in enumerate(moved)]
    for c in copies:
        c.start()
    shards = (w0,) + tuple(wv.at[i] for i in range(7))

    def lower(c, start, stop):
        return shards[2 * c][start:stop, :]

    def upper(c, start, stop):
        return shards[2 * c + 1][start - RELAYED : stop - RELAYED, :]

    tokens = side([rows[i] for i in range(4)])
    hidden = []
    for c in range(4):
        for i in ((0,), (1, 2), (3, 4), (5, 6))[c]:
            copies[i].wait()
        ups = [lower(c, UP_AT, RELAYED), upper(c, RELAYED, DOWN_AT)]
        both = side([lower(c, 0, UP_AT), jnp.concatenate(ups, axis=0)])
        parts = jnp.dot(tokens, both, preferred_element_type=F32)
        hidden.append((jax.nn.silu(parts[:, :LANES]) * parts[:, LANES:]).astype(BF16))
    hidden = side(hidden)

    def block(c, b):
        return upper(c, DOWN_AT + b * LANES, DOWN_AT + (b + 1) * LANES)

    sends = []
    for b in range(0, 16, 2):
        down = jnp.concatenate([side([block(c, b), block(c, b + 1)]) for c in range(4)], axis=0)
        part = jnp.dot(hidden, down, preferred_element_type=F32).astype(BF16)
        part_v[b] = part[:, :LANES]
        part_v[b + 1] = part[:, LANES:]
        target = out.at[pl.ds(b, 2), pl.ds(0, ROUTED_ROWS), :]
        sends.append(pltpu.make_async_copy(part_v.at[pl.ds(b, 2)], target, sems.at[7 + b // 2]))
        sends[-1].start()
    for c in sends:
        c.wait()


def return_body(parts, send, shared):
    routed = []
    for x in range(4):
        total = parts[x, 0:ROUTED_ROWS, :].astype(F32)
        for y in range(1, 4):
            total = total + parts[4 * y + x, 0:ROUTED_ROWS, :].astype(F32)
        routed.append(total.astype(BF16))
    for half in range(2):
        total = jnp.zeros((SHARED_ROWS, LANES), F32)
        for y in (half, half + 2):
            for x in range(4):
                total = total + parts[4 * y + x, ROUTED_ROWS:, :].astype(F32)
        shared[half * SHARED_ROWS : (half + 1) * SHARED_ROWS, :] = total
    rows = jnp.concatenate(routed, axis=0)
    count = 4 * ROUTED_ROWS
    came = iota((1, count), 1)
    x = (
        (came >= ROUTED_ROWS).astype(jnp.int32)
        + (came >= 2 * ROUTED_ROWS).astype(jnp.int32)
        + (came >= 3 * ROUTED_ROWS).astype(jnp.int32)
    )
    within = came - ROUTED_ROWS * x
    source = (within * 10923) >> 16
    goes = 18 * source + 6 * x + within
    move = chosen(iota((count, count), 0) == goes)
    send[...] = jnp.dot(move, rows, preferred_element_type=F32).astype(BF16)


def weigh_body(routes, weight, high_out, low_out):
    named = routes[...]
    scale = weight[...]
    slot = iota((4 * ROUTED_ROWS, TOKENS_HERE), 0)
    taken = jnp.zeros(slot.shape, F32)
    for k, rank in enumerate(ranks_of(named)):
        at = named[k : k + 1] * (4 * SLOTS_USED) + SLOTS_USED * (rank & 3) + (rank >> 2)
        taken = jnp.where(slot == at, scale[k : k + 1], taken)
    taken = taken.T
    high = taken.astype(BF16)
    high_out[...] = high
    low_out[...] = (taken - high.astype(F32)).astype(BF16)


def combine_body(rows, high, low, own, shared, second_out, stats_out):
    mix = jnp.dot(high[...], rows[...], preferred_element_type=F32)
    mix = mix + jnp.dot(low[...], rows[...], preferred_element_type=F32)
    second = RESIDUAL_SCALE * own[...].astype(F32) + mix + shared[...]
    second_out[...] = second
    stats = row_stats(second)[0:2]
    for i in range(16):
        stats_out[i] = stats


def settle_body(second, stats, gain, bias, out):
    total = stats[0]
    for i in range(1, 16):
        total = total + stats[i]
    mean, inv = mean_and_scale(total)
    out[...] = ((second[...] - mean) * inv * gain[...] + bias[...]).astype(BF16)


def struct(shape, dtype):
    return pltpu.HBM(shape, dtype)


def held(shape, dtype):
    return pltpu.VMEM(shape, dtype)


def exchange(parts, axes):
    return lax.all_to_all(parts, axes, split_axis=0, concat_axis=0, tiled=True)


def around(shard, by):
    return lax.ppermute(shard, "x", [(i, (i + by) % 4) for i in range(4)])


def kernel(body, in_specs, **options):
    params = pltpu.CompilerParams(vmem_limit_bytes=24 * 1024 * 1024)
    call = pl.pallas_call(body, in_specs=in_specs, compiler_params=params, **options)
    places = {id(HELD): pltpu.VMEM, id(HBM): pltpu.HBM}

    def run(*args):
        args = [
            pltpu.with_memory_space_constraint(a, places[id(s)]) if id(s) in places else a
            for a, s in zip(args, in_specs, strict=True)
        ]
        return call(*args)

    return run


def layer(
    layer_input,
    doc_ids,
    routes,
    route_weight,
    pool_weight,
    pool_scale,
    norm1_gain,
    norm1_bias,
    expert_gate,
    expert_up,
    expert_down,
    shared_gate,
    shared_up,
    shared_down,
    norm2_gain,
    norm2_bias,
):
    core = lax.axis_index("sp") & 1
    at = jnp.stack([lax.axis_index("y"), lax.axis_index("x"), core]).astype(jnp.int32)
    spread = kernel(
        spread_body,
        out_shape=struct((16, TOKENS_HERE, LANES), BF16),
        in_specs=[HBM],
        out_specs=HBM,
        scratch_shapes=[
            pltpu.VMEM((TOKENS_HERE, LANES), BF16),
            pltpu.SemaphoreType.DMA((17,)),
        ],
    )(layer_input)
    near = exchange(spread, ("y", "x"))
    low, high, shared_packed, shared_half = kernel(
        pack_body,
        out_shape=[
            held((RELAYED, LANES), BF16),
            held((RELAYED, LANES), BF16),
            struct((3 * SHARED_UNITS, MODEL), BF16),
            struct((3 * HALF_UNITS, MODEL), BF16),
        ],
        in_specs=[SMEM] + [HBM] * 6,
        out_specs=[VMEM] * 4,
        scratch_shapes=[pltpu.SemaphoreType.DMA((25,))],
        cost_estimate=pl.CostEstimate(
            flops=10_000_000, bytes_accessed=4 * PACKED * LANES, transcendentals=0
        ),
    )(
        at,
        expert_gate[0],
        expert_up[0],
        expert_down[0],
        shared_gate.T,
        shared_up.T,
        shared_down,
    )
    marks = jnp.broadcast_to((doc_ids[-HALO:] + 1).astype(BF16)[:, None], (HALO, LANES))
    tail = jnp.concatenate([near[:, -HALO:, :], marks[None]], axis=0)
    following = [(i, i + 1) for i in range(lax.axis_size("sp") - 1)]
    halo = lax.ppermute(tail, "sp", following)
    left_low = around(low, 1)
    right_high = around(high, -1)
    left_high = around(high, 1)
    right_low = around(low, -1)
    send, normed, own = kernel(
        mixer_body,
        in_specs=[SMEM] + [VMEM] * 5 + [HELD, HELD, HBM],
        out_specs=[HBM, VMEM, VMEM],
        scratch_shapes=[
            pltpu.VMEM((4, QUARTER, QUARTER), BF16),
            pltpu.VMEM((4, TOKENS_HERE, QUARTER), BF16),
            pltpu.VMEM((4, TOKENS_HERE, QUARTER), F32),
            pltpu.VMEM((TOKENS_HERE, QUARTER), BF16),
            pltpu.VMEM((EXPERTS * SLOTS_SENT, QUARTER), BF16),
            pltpu.SemaphoreType.DMA((5,)),
        ],
        out_shape=[
            struct((EXPERTS * SLOTS_SENT, QUARTER), BF16),
            held((4, SHARED_ROWS, QUARTER), BF16),
            held((TOKENS_HERE, LANES), BF16),
        ],
    )(
        at,
        doc_ids[None],
        routes.T,
        pool_scale[None],
        norm1_gain[None],
        norm1_bias[None],
        near,
        halo,
        pool_weight,
    )
    from_pair = lax.ppermute(shared_half, "y", [(i, i ^ 1) for i in range(4)])
    cores = [(i, i ^ 1) for i in range(lax.axis_size("sp"))]
    from_core = lax.ppermute(from_pair, "sp", cores)
    across_low = around(left_low, 1)
    across_high = around(right_high, -1)
    arrived = exchange(send.reshape(EXPERTS, SLOTS_SENT, QUARTER), "sp")
    gather_in = kernel(
        compact_body,
        out_shape=struct((4, ROUTED_ROWS, QUARTER), BF16),
        in_specs=[HELD],
        out_specs=VMEM,
    )(arrived.reshape(EXPERTS * SLOTS_SENT, QUARTER))
    gathered = exchange(gather_in, "y")
    begun = kernel(
        shared_body,
        out_shape=struct((16, ROUTED_ROWS + SHARED_ROWS, LANES), BF16),
        in_specs=[HELD, HBM, HBM, ANY],
        out_specs=HBM,
        scratch_shapes=[
            pltpu.VMEM((3 * SHARED_UNITS, MODEL), BF16),
            pltpu.VMEM((3 * HALF_UNITS, MODEL), BF16),
            pltpu.VMEM((3 * HALF_UNITS, MODEL), BF16),
            pltpu.VMEM((16, SHARED_ROWS, LANES), BF16),
            pltpu.SemaphoreType.DMA((4,)),
        ],
    )(normed, shared_packed, from_pair, from_core)
    partial = kernel(
        expert_body,
        out_shape=struct((16, ROUTED_ROWS + SHARED_ROWS, LANES), BF16),
        in_specs=[HELD] * 2 + [HBM] * 8,
        out_specs=HBM,
        scratch_shapes=[
            pltpu.VMEM((7, RELAYED, LANES), BF16),
            pltpu.VMEM((16, ROUTED_ROWS, LANES), BF16),
            pltpu.SemaphoreType.DMA((15,)),
        ],
        input_output_aliases={9: 0},
    )(
        gathered,
        low,
        high,
        left_low,
        left_high,
        right_low,
        right_high,
        across_low,
        across_high,
        begun,
    )
    parts = exchange(partial, ("y", "x"))
    back, shared_sum = kernel(
        return_body,
        out_shape=[
            struct((4 * ROUTED_ROWS, LANES), BF16),
            held((TOKENS_HERE, LANES), F32),
        ],
        in_specs=[HELD],
        out_specs=[VMEM, VMEM],
    )(parts)
    returned = exchange(back.reshape(EXPERTS, 4 * SLOTS_USED, LANES), "sp")
    high_weights, low_weights = kernel(
        weigh_body,
        out_shape=[held((TOKENS_HERE, 4 * ROUTED_ROWS), BF16)] * 2,
        in_specs=[VMEM] * 2,
        out_specs=[VMEM] * 2,
    )(routes.T, route_weight.T)
    second, row_sums = kernel(
        combine_body,
        out_shape=[held((TOKENS_HERE, LANES), F32), struct((16, 2, TOKENS_HERE), F32)],
        in_specs=[HELD] * 5,
        out_specs=[VMEM, VMEM],
    )(returned.reshape(4 * ROUTED_ROWS, LANES), high_weights, low_weights, own, shared_sum)
    row_sums = exchange(row_sums, ("y", "x"))
    return kernel(
        settle_body,
        out_shape=jax.ShapeDtypeStruct((TOKENS_HERE, LANES), BF16),
        in_specs=[HELD, HELD, VMEM, VMEM],
        out_specs=VMEM,
    )(second, row_sums, norm2_gain[None], norm2_bias[None])


def solution(mesh):
    split = Mesh(mesh.devices.reshape(mesh.shape["sp"], 4, 4), ("sp", "y", "x"))
    tp = ("y", "x")
    placed = (
        P("sp", tp),
        P("sp"),
        P("sp", None),
        P("sp", None),
        P(),
        P(),
        P(),
        P(),
        P("sp", None, tp),
        P("sp", None, tp),
        P("sp", tp, None),
        P(None, tp),
        P(None, tp),
        P(tp, None),
        P(tp),
        P(tp),
    )
    return jax.shard_map(layer, mesh=split, in_specs=placed, out_specs=P("sp", tp), check_vma=False)
```

```python
import jax
import jax.numpy as jnp
from jax import lax
from jax.experimental import pallas as pl
from jax.experimental.pallas import tpu as pltpu
from jax.sharding import Mesh
from jax.sharding import PartitionSpec as P


RESIDUAL_SCALE = 2.0**0.5
NORM_EPS = 1e-05
HALO = 16
F32 = jnp.float32
BF16 = jnp.bfloat16
VMEM = pl.BlockSpec(memory_space=pltpu.VMEM)
HELD = pl.BlockSpec(memory_space=pltpu.VMEM)
HBM = pl.BlockSpec(memory_space=pltpu.HBM)
ANY = pl.BlockSpec(memory_space=pl.ANY)
SMEM = pl.BlockSpec(memory_space=pltpu.SMEM)

TOKENS_HERE = 256
EXPERTS = 32
LANES = 128
QUARTER = 512
MODEL = 2048
SLOTS_SENT = 8
SLOTS_USED = 6
ROUTED_ROWS = EXPERTS * SLOTS_USED
SHARED_ROWS = 128
UP_AT = 2048
DOWN_AT = 4096
PACKED = 6144
SHARED_UNITS = 64
HALF_UNITS = SHARED_UNITS // 2
RELAYED = PACKED // 2


def iota(shape, dim):
    return lax.broadcasted_iota(jnp.int32, shape, dim)


def side(parts):
    return jnp.concatenate(parts, axis=1)


def as_column(row):
    return jnp.broadcast_to(row, (LANES, row.shape[1])).T


def chosen(mask):
    return mask.astype(F32).astype(BF16)


def sums(values):
    total = jnp.sum(values, axis=1, keepdims=True)
    return total, jnp.sum(values * values, axis=1, keepdims=True)


def row_stats(values):
    lane = iota((values.shape[0], LANES), 1)
    total, squares = sums(values)
    return jnp.where(lane == 0, total, jnp.where(lane == 1, squares, 0.0)).T


def mean_and_scale(total):
    mean = total[0:1] / MODEL
    var = total[1:2] / MODEL - mean * mean
    return as_column(mean), as_column(lax.rsqrt(var + NORM_EPS))


def ranks_of(routes):
    expert = iota((EXPERTS, TOKENS_HERE), 0)
    picks = [routes[k : k + 1] == expert for k in range(2)]
    named = chosen(picks[0] | picks[1])
    earlier = chosen(iota((TOKENS_HERE, TOKENS_HERE), 0) < iota((TOKENS_HERE, TOKENS_HERE), 1))
    counts = jnp.dot(named, earlier, preferred_element_type=F32)
    return [
        jnp.sum(jnp.where(p, counts, 0.0), axis=0, keepdims=True).astype(jnp.int32) for p in picks
    ]


def pack_body(at, gate, up, down, sgate, sup, sdown, low, high, shared_out, half_out, sems):
    core = pl.multiple_of(at[2] * HALF_UNITS, HALF_UNITS)
    rest = DOWN_AT - RELAYED
    plan = [
        (gate, low.at[pl.ds(0, UP_AT)]),
        (up.at[pl.ds(0, RELAYED - UP_AT)], low.at[pl.ds(UP_AT, RELAYED - UP_AT)]),
        (up.at[pl.ds(RELAYED - UP_AT, rest)], high.at[pl.ds(0, rest)]),
    ]
    for b in range(16):
        lanes = pl.ds(b * LANES, LANES)
        plan.append((down.at[:, lanes], high.at[pl.ds(rest + b * LANES, LANES)]))
    for i, part in enumerate((sgate, sup, sdown)):
        plan.append((part, shared_out.at[pl.ds(i * SHARED_UNITS, SHARED_UNITS)]))
        mine = part.at[pl.ds(core, HALF_UNITS)]
        plan.append((mine, half_out.at[pl.ds(i * HALF_UNITS, HALF_UNITS)]))
    copies = [pltpu.make_async_copy(s, d, sems.at[i]) for i, (s, d) in enumerate(plan)]
    for c in copies:
        c.start()
    for c in copies:
        c.wait()


def spread_body(shard, out, block, sems):
    move = pltpu.make_async_copy(shard, block, sems.at[16])
    move.start()
    move.wait()
    copies = [pltpu.make_async_copy(block, out.at[i], sems.at[i]) for i in range(16)]
    for c in copies:
        c.start()
    for c in copies:
        c.wait()


def mixer_body(
    at,
    docs,
    routes,
    scale,
    gain,
    bias,
    near,
    halo,
    weight,
    send,
    normed,
    own,
    weight_v,
    mixed_v,
    first_v,
    quarter_v,
    send_v,
    sems,
):
    y, x = at[0], at[1]
    copies = [pltpu.make_async_copy(weight.at[g], weight_v.at[g], sems.at[g]) for g in range(4)]
    for c in copies:
        c.start()
    own_row = (docs[...] + 1).astype(F32)
    own_marks = as_column(own_row)
    halo_row = halo[16].astype(F32).T[0:1]
    apart = iota((TOKENS_HERE, TOKENS_HERE), 0) - iota((TOKENS_HERE, TOKENS_HERE), 1)
    inside = (side([own_marks, own_marks]) == own_row) & (apart >= 0)
    corner = iota((HALO, HALO), 0) - iota((HALO, HALO), 1) + HALO
    corner_inside = own_marks[0:HALO, 0:HALO] == halo_row
    for g in range(4):
        window = 2 << g
        band = jnp.where(inside & (apart < window), 1.0, 0.0)
        edge = jnp.where(corner_inside & (corner < window), 1.0, 0.0)
        members = jnp.sum(band, axis=1, keepdims=True)
        first_members = members[0:HALO] + jnp.sum(edge, axis=1, keepdims=True)
        scale_by = 1.0 / jnp.concatenate([first_members, members[HALO:]], axis=0)
        band, edge = band.astype(BF16), edge.astype(BF16)
        for j in range(2):
            at_lane = slice(j * 2 * LANES, (j + 1) * 2 * LANES)
            mine = side([near[4 * g + 2 * j], near[4 * g + 2 * j + 1]])
            head = side([halo[4 * g + 2 * j], halo[4 * g + 2 * j + 1]])
            running = jnp.dot(band, mine, preferred_element_type=F32)
            begin = running[0:HALO] + jnp.dot(edge, head, preferred_element_type=F32)
            running = jnp.concatenate([begin, running[HALO:]], axis=0)
            mixed_v[g, :, at_lane] = (running * scale_by - mine.astype(F32)).astype(BF16)
    total = jnp.zeros((TOKENS_HERE, 1), F32)
    squares = jnp.zeros((TOKENS_HERE, 1), F32)
    for g in range(4):
        copies[g].wait()
        for j in range(2):
            at_lane = slice(j * 2 * LANES, (j + 1) * 2 * LANES)
            lanes = slice(g * QUARTER + j * 2 * LANES, g * QUARTER + (j + 1) * 2 * LANES)
            projected = jnp.dot(mixed_v[g], weight_v[g, :, at_lane], preferred_element_type=F32)
            mine = side([near[4 * g + 2 * j], near[4 * g + 2 * j + 1]]).astype(F32)
            first = RESIDUAL_SCALE * mine + projected * scale[:, lanes]
            first_v[g, :, at_lane] = first
            part, part_squares = sums(first)
            total = total + part
            squares = squares + part_squares
    mean = total / MODEL
    inv = lax.rsqrt(squares / MODEL - mean * mean + NORM_EPS)
    lanes = pl.ds(pl.multiple_of(y * QUARTER, QUARTER), QUARTER)
    gain_here, bias_here = gain[:, lanes], bias[:, lanes]
    for r in range(0, TOKENS_HERE, 64):
        rows = slice(r, r + 64)
        scaled = (first_v[y, rows, :] - mean[rows]) * inv[rows]
        quarter_v[rows, :] = (scaled * gain_here + bias_here).astype(BF16)
    quarter = quarter_v[...]
    named = routes[...]
    dests = []
    for k, rank in enumerate(ranks_of(named)):
        slot = named[k : k + 1] * SLOTS_SENT + (rank >> 2)
        dests.append(jnp.where((rank & 3) == x, slot, -1))
    slot = iota((EXPERTS * SLOTS_SENT, TOKENS_HERE), 0)
    pick = chosen((slot == dests[0]) | (slot == dests[1]))
    send_v[...] = jnp.dot(pick, quarter, preferred_element_type=F32).astype(BF16)
    leave = pltpu.make_async_copy(send_v, send, sems.at[4])
    leave.start()
    mine = quarter[:, 0:LANES]
    for i in range(1, 4):
        mine = jnp.where(x == i, quarter[:, i * LANES : (i + 1) * LANES], mine)
    own[...] = mine
    upper = (y & 1) == 1
    half = pl.multiple_of((y & 1) * SHARED_ROWS, SHARED_ROWS)
    mean = jnp.where(upper, mean[SHARED_ROWS:], mean[:SHARED_ROWS])
    inv = jnp.where(upper, inv[SHARED_ROWS:], inv[:SHARED_ROWS])
    for r in range(0, SHARED_ROWS, 64):
        rows = slice(r, r + 64)
        for g in range(4):
            lanes = slice(g * QUARTER, (g + 1) * QUARTER)
            scaled = (first_v[g, pl.ds(half + r, 64), :] - mean[rows]) * inv[rows]
            normed[g, rows, :] = (scaled * gain[:, lanes] + bias[:, lanes]).astype(BF16)
    leave.wait()


def compact_body(rows, out):
    shape = (ROUTED_ROWS, EXPERTS * SLOTS_SENT)
    came = iota(shape, 1)
    within = came & 7
    goes = SLOTS_USED * (came >> 3) + within
    keep = chosen((iota(shape, 0) == goes) & (within < SLOTS_USED))
    packed = jnp.dot(keep, rows[...], preferred_element_type=F32).astype(BF16)
    for i in range(4):
        out[i] = packed


def shared_body(normed, s0, s1, s2, out, own_v, near_v, far_v, part_v, sems):
    copies = [
        pltpu.make_async_copy(source, target, sems.at[i])
        for i, (source, target) in enumerate(((s0, own_v), (s1, near_v), (s2, far_v)))
    ]
    for c in copies:
        c.start()
    shared = side([normed[i] for i in range(4)])
    for c in copies:
        c.wait()

    def units(i, lanes):
        here = slice(i * SHARED_UNITS, (i + 1) * SHARED_UNITS)
        half = slice(i * HALF_UNITS, (i + 1) * HALF_UNITS)
        return jnp.concatenate([own_v[here, lanes], near_v[half, lanes], far_v[half, lanes]], axis=0)

    contract = (((1,), (1,)), ((), ()))
    every = slice(0, MODEL)
    sg = lax.dot_general(shared, units(0, every), contract, preferred_element_type=F32)
    su = lax.dot_general(shared, units(1, every), contract, preferred_element_type=F32)
    hidden = (jax.nn.silu(sg) * su).astype(BF16)
    for b in range(0, 16, 2):
        down = units(2, slice(b * LANES, (b + 2) * LANES))
        part = jnp.dot(hidden, down, preferred_element_type=F32).astype(BF16)
        part_v[b] = part[:, :LANES]
        part_v[b + 1] = part[:, LANES:]
    send = pltpu.make_async_copy(part_v, out.at[:, pl.ds(ROUTED_ROWS, SHARED_ROWS), :], sems.at[3])
    send.start()
    send.wait()


def expert_body(rows, w0, w1, w2, w3, w4, w5, w6, w7, begun, out, wv, part_v, sems):
    moved = (w2, w3, w4, w5, w6, w7)
    copies = [pltpu.make_async_copy(m, wv.at[i], sems.at[i]) for i, m in enumerate(moved)]
    for c in copies:
        c.start()
    shards = (w0, w1) + tuple(wv.at[i] for i in range(6))

    def lower(c, start, stop):
        return shards[2 * c][start:stop, :]

    def upper(c, start, stop):
        return shards[2 * c + 1][start - RELAYED : stop - RELAYED, :]

    tokens = side([rows[i] for i in range(4)])
    hidden = []
    for c in range(4):
        for i in ((), (0, 1), (2, 3), (4, 5))[c]:
            copies[i].wait()
        ups = [lower(c, UP_AT, RELAYED), upper(c, RELAYED, DOWN_AT)]
        both = side([lower(c, 0, UP_AT), jnp.concatenate(ups, axis=0)])
        parts = jnp.dot(tokens, both, preferred_element_type=F32)
        hidden.append((jax.nn.silu(parts[:, :LANES]) * parts[:, LANES:]).astype(BF16))
    hidden = side(hidden)

    def block(c, b):
        return upper(c, DOWN_AT + b * LANES, DOWN_AT + (b + 1) * LANES)

    sends = []
    for b in range(0, 16, 2):
        down = jnp.concatenate([side([block(c, b), block(c, b + 1)]) for c in range(4)], axis=0)
        part = jnp.dot(hidden, down, preferred_element_type=F32).astype(BF16)
        part_v[b] = part[:, :LANES]
        part_v[b + 1] = part[:, LANES:]
        target = out.at[pl.ds(b, 2), pl.ds(0, ROUTED_ROWS), :]
        sends.append(pltpu.make_async_copy(part_v.at[pl.ds(b, 2)], target, sems.at[6 + b // 2]))
        sends[-1].start()
    for c in sends:
        c.wait()


def return_body(parts, send, shared):
    routed = []
    for x in range(4):
        total = parts[x, 0:ROUTED_ROWS, :].astype(F32)
        for y in range(1, 4):
            total = total + parts[4 * y + x, 0:ROUTED_ROWS, :].astype(F32)
        routed.append(total.astype(BF16))
    for half in range(2):
        total = jnp.zeros((SHARED_ROWS, LANES), F32)
        for y in (half, half + 2):
            for x in range(4):
                total = total + parts[4 * y + x, ROUTED_ROWS:, :].astype(F32)
        shared[half * SHARED_ROWS : (half + 1) * SHARED_ROWS, :] = total
    rows = jnp.concatenate(routed, axis=0)
    count = 4 * ROUTED_ROWS
    came = iota((1, count), 1)
    x = (
        (came >= ROUTED_ROWS).astype(jnp.int32)
        + (came >= 2 * ROUTED_ROWS).astype(jnp.int32)
        + (came >= 3 * ROUTED_ROWS).astype(jnp.int32)
    )
    within = came - ROUTED_ROWS * x
    source = (within * 10923) >> 16
    goes = 18 * source + 6 * x + within
    move = chosen(iota((count, count), 0) == goes)
    send[...] = jnp.dot(move, rows, preferred_element_type=F32).astype(BF16)


def weigh_body(routes, weight, high_out, low_out):
    named = routes[...]
    scale = weight[...]
    slot = iota((4 * ROUTED_ROWS, TOKENS_HERE), 0)
    taken = jnp.zeros(slot.shape, F32)
    for k, rank in enumerate(ranks_of(named)):
        at = named[k : k + 1] * (4 * SLOTS_USED) + SLOTS_USED * (rank & 3) + (rank >> 2)
        taken = jnp.where(slot == at, scale[k : k + 1], taken)
    taken = taken.T
    high = taken.astype(BF16)
    high_out[...] = high
    low_out[...] = (taken - high.astype(F32)).astype(BF16)


def combine_body(rows, high, low, own, shared, second_out, stats_out):
    mix = jnp.dot(high[...], rows[...], preferred_element_type=F32)
    mix = mix + jnp.dot(low[...], rows[...], preferred_element_type=F32)
    second = RESIDUAL_SCALE * own[...].astype(F32) + mix + shared[...]
    second_out[...] = second
    stats = row_stats(second)[0:2]
    for i in range(16):
        stats_out[i] = stats


def settle_body(second, stats, gain, bias, out):
    total = stats[0]
    for i in range(1, 16):
        total = total + stats[i]
    mean, inv = mean_and_scale(total)
    out[...] = ((second[...] - mean) * inv * gain[...] + bias[...]).astype(BF16)


def struct(shape, dtype):
    return pltpu.HBM(shape, dtype)


def held(shape, dtype):
    return pltpu.VMEM(shape, dtype)


def exchange(parts, axes):
    return lax.all_to_all(parts, axes, split_axis=0, concat_axis=0, tiled=True)


def around(shard, by):
    return lax.ppermute(shard, "x", [(i, (i + by) % 4) for i in range(4)])


def kernel(body, in_specs, **options):
    params = pltpu.CompilerParams(vmem_limit_bytes=24 * 1024 * 1024)
    call = pl.pallas_call(body, in_specs=in_specs, compiler_params=params, **options)
    places = {id(HELD): pltpu.VMEM, id(HBM): pltpu.HBM}

    def run(*args):
        args = [
            pltpu.with_memory_space_constraint(a, places[id(s)]) if id(s) in places else a
            for a, s in zip(args, in_specs, strict=True)
        ]
        return call(*args)

    return run


def layer(
    layer_input,
    doc_ids,
    routes,
    route_weight,
    pool_weight,
    pool_scale,
    norm1_gain,
    norm1_bias,
    expert_gate,
    expert_up,
    expert_down,
    shared_gate,
    shared_up,
    shared_down,
    norm2_gain,
    norm2_bias,
):
    core = lax.axis_index("sp") & 1
    at = jnp.stack([lax.axis_index("y"), lax.axis_index("x"), core]).astype(jnp.int32)
    spread = kernel(
        spread_body,
        out_shape=struct((16, TOKENS_HERE, LANES), BF16),
        in_specs=[HBM],
        out_specs=HBM,
        scratch_shapes=[
            pltpu.VMEM((TOKENS_HERE, LANES), BF16),
            pltpu.SemaphoreType.DMA((17,)),
        ],
    )(layer_input)
    near = exchange(spread, ("y", "x"))
    low, high, shared_packed, shared_half = kernel(
        pack_body,
        out_shape=[
            held((RELAYED, LANES), BF16),
            held((RELAYED, LANES), BF16),
            struct((3 * SHARED_UNITS, MODEL), BF16),
            struct((3 * HALF_UNITS, MODEL), BF16),
        ],
        in_specs=[SMEM] + [HBM] * 6,
        out_specs=[VMEM] * 4,
        scratch_shapes=[pltpu.SemaphoreType.DMA((25,))],
        cost_estimate=pl.CostEstimate(
            flops=10_000_000, bytes_accessed=4 * PACKED * LANES, transcendentals=0
        ),
    )(
        at,
        expert_gate[0],
        expert_up[0],
        expert_down[0],
        shared_gate.T,
        shared_up.T,
        shared_down,
    )
    marks = jnp.broadcast_to((doc_ids[-HALO:] + 1).astype(BF16)[:, None], (HALO, LANES))
    tail = jnp.concatenate([near[:, -HALO:, :], marks[None]], axis=0)
    following = [(i, i + 1) for i in range(lax.axis_size("sp") - 1)]
    halo = lax.ppermute(tail, "sp", following)
    left_low = around(low, 1)
    right_high = around(high, -1)
    left_high = around(high, 1)
    right_low = around(low, -1)
    send, normed, own = kernel(
        mixer_body,
        in_specs=[SMEM] + [VMEM] * 5 + [HELD, HELD, HBM],
        out_specs=[HBM, VMEM, VMEM],
        scratch_shapes=[
            pltpu.VMEM((4, QUARTER, QUARTER), BF16),
            pltpu.VMEM((4, TOKENS_HERE, QUARTER), BF16),
            pltpu.VMEM((4, TOKENS_HERE, QUARTER), F32),
            pltpu.VMEM((TOKENS_HERE, QUARTER), BF16),
            pltpu.VMEM((EXPERTS * SLOTS_SENT, QUARTER), BF16),
            pltpu.SemaphoreType.DMA((5,)),
        ],
        out_shape=[
            struct((EXPERTS * SLOTS_SENT, QUARTER), BF16),
            held((4, SHARED_ROWS, QUARTER), BF16),
            held((TOKENS_HERE, LANES), BF16),
        ],
    )(
        at,
        doc_ids[None],
        routes.T,
        pool_scale[None],
        norm1_gain[None],
        norm1_bias[None],
        near,
        halo,
        pool_weight,
    )
    from_pair = lax.ppermute(shared_half, "y", [(i, i ^ 1) for i in range(4)])
    cores = [(i, i ^ 1) for i in range(lax.axis_size("sp"))]
    from_core = lax.ppermute(from_pair, "sp", cores)
    across_low = around(left_low, 1)
    across_high = around(right_high, -1)
    arrived = exchange(send.reshape(EXPERTS, SLOTS_SENT, QUARTER), "sp")
    gather_in = kernel(
        compact_body,
        out_shape=struct((4, ROUTED_ROWS, QUARTER), BF16),
        in_specs=[HELD],
        out_specs=VMEM,
    )(arrived.reshape(EXPERTS * SLOTS_SENT, QUARTER))
    gathered = exchange(gather_in, "y")
    begun = kernel(
        shared_body,
        out_shape=struct((16, ROUTED_ROWS + SHARED_ROWS, LANES), BF16),
        in_specs=[HELD, HBM, HBM, ANY],
        out_specs=HBM,
        scratch_shapes=[
            pltpu.VMEM((3 * SHARED_UNITS, MODEL), BF16),
            pltpu.VMEM((3 * HALF_UNITS, MODEL), BF16),
            pltpu.VMEM((3 * HALF_UNITS, MODEL), BF16),
            pltpu.VMEM((16, SHARED_ROWS, LANES), BF16),
            pltpu.SemaphoreType.DMA((4,)),
        ],
    )(normed, shared_packed, from_pair, from_core)
    partial = kernel(
        expert_body,
        out_shape=struct((16, ROUTED_ROWS + SHARED_ROWS, LANES), BF16),
        in_specs=[HELD] * 3 + [HBM] * 7,
        out_specs=HBM,
        scratch_shapes=[
            pltpu.VMEM((6, RELAYED, LANES), BF16),
            pltpu.VMEM((16, ROUTED_ROWS, LANES), BF16),
            pltpu.SemaphoreType.DMA((14,)),
        ],
        input_output_aliases={9: 0},
    )(
        gathered,
        low,
        high,
        left_low,
        left_high,
        right_low,
        right_high,
        across_low,
        across_high,
        begun,
    )
    parts = exchange(partial, ("y", "x"))
    back, shared_sum = kernel(
        return_body,
        out_shape=[
            struct((4 * ROUTED_ROWS, LANES), BF16),
            held((TOKENS_HERE, LANES), F32),
        ],
        in_specs=[HELD],
        out_specs=[VMEM, VMEM],
    )(parts)
    returned = exchange(back.reshape(EXPERTS, 4 * SLOTS_USED, LANES), "sp")
    high_weights, low_weights = kernel(
        weigh_body,
        out_shape=[held((TOKENS_HERE, 4 * ROUTED_ROWS), BF16)] * 2,
        in_specs=[VMEM] * 2,
        out_specs=[VMEM] * 2,
    )(routes.T, route_weight.T)
    second, row_sums = kernel(
        combine_body,
        out_shape=[held((TOKENS_HERE, LANES), F32), struct((16, 2, TOKENS_HERE), F32)],
        in_specs=[HELD] * 5,
        out_specs=[VMEM, VMEM],
    )(returned.reshape(4 * ROUTED_ROWS, LANES), high_weights, low_weights, own, shared_sum)
    row_sums = exchange(row_sums, ("y", "x"))
    return kernel(
        settle_body,
        out_shape=jax.ShapeDtypeStruct((TOKENS_HERE, LANES), BF16),
        in_specs=[HELD, HELD, VMEM, VMEM],
        out_specs=VMEM,
    )(second, row_sums, norm2_gain[None], norm2_bias[None])


def solution(mesh):
    split = Mesh(mesh.devices.reshape(mesh.shape["sp"], 4, 4), ("sp", "y", "x"))
    tp = ("y", "x")
    placed = (
        P("sp", tp),
        P("sp"),
        P("sp", None),
        P("sp", None),
        P(),
        P(),
        P(),
        P(),
        P("sp", None, tp),
        P("sp", None, tp),
        P("sp", tp, None),
        P(None, tp),
        P(None, tp),
        P(tp, None),
        P(tp),
        P(tp),
    )
    return jax.shard_map(layer, mesh=split, in_specs=placed, out_specs=P("sp", tp), check_vma=False)
```

```python
import jax
import jax.numpy as jnp
from jax import lax
from jax.experimental import pallas as pl
from jax.experimental.pallas import tpu as pltpu
from jax.sharding import Mesh
from jax.sharding import PartitionSpec as P


RESIDUAL_SCALE = 2.0**0.5
NORM_EPS = 1e-05
HALO = 16
F32 = jnp.float32
BF16 = jnp.bfloat16
VMEM = pl.BlockSpec(memory_space=pltpu.VMEM)
HELD = pl.BlockSpec(memory_space=pltpu.VMEM)
HBM = pl.BlockSpec(memory_space=pltpu.HBM)
ANY = pl.BlockSpec(memory_space=pl.ANY)
SMEM = pl.BlockSpec(memory_space=pltpu.SMEM)

TOKENS_HERE = 256
EXPERTS = 32
LANES = 128
QUARTER = 512
MODEL = 2048
SLOTS_SENT = 8
SLOTS_USED = 6
ROUTED_ROWS = EXPERTS * SLOTS_USED
SHARED_ROWS = 128
UP_AT = 2048
DOWN_AT = 4096
PACKED = 6144
SHARED_UNITS = 64
HALF_UNITS = SHARED_UNITS // 2
RELAYED = PACKED // 2


def iota(shape, dim):
    return lax.broadcasted_iota(jnp.int32, shape, dim)


def side(parts):
    return jnp.concatenate(parts, axis=1)


def as_column(row):
    return jnp.broadcast_to(row, (LANES, row.shape[1])).T


def chosen(mask):
    return mask.astype(F32).astype(BF16)


def sums(values):
    total = jnp.sum(values, axis=1, keepdims=True)
    return total, jnp.sum(values * values, axis=1, keepdims=True)


def row_stats(values):
    lane = iota((values.shape[0], LANES), 1)
    total, squares = sums(values)
    return jnp.where(lane == 0, total, jnp.where(lane == 1, squares, 0.0)).T


def mean_and_scale(total):
    mean = total[0:1] / MODEL
    var = total[1:2] / MODEL - mean * mean
    return as_column(mean), as_column(lax.rsqrt(var + NORM_EPS))


def ranks_of(routes):
    expert = iota((EXPERTS, TOKENS_HERE), 0)
    picks = [routes[k : k + 1] == expert for k in range(2)]
    named = chosen(picks[0] | picks[1])
    earlier = chosen(iota((TOKENS_HERE, TOKENS_HERE), 0) < iota((TOKENS_HERE, TOKENS_HERE), 1))
    counts = jnp.dot(named, earlier, preferred_element_type=F32)
    return [
        jnp.sum(jnp.where(p, counts, 0.0), axis=0, keepdims=True).astype(jnp.int32) for p in picks
    ]


def pack_body(at, gate, up, down, sgate, sup, sdown, low, high, shared_out, half_out, sems):
    core = pl.multiple_of(at[2] * HALF_UNITS, HALF_UNITS)
    rest = DOWN_AT - RELAYED
    plan = [
        (gate, low.at[pl.ds(0, UP_AT)]),
        (up.at[pl.ds(0, RELAYED - UP_AT)], low.at[pl.ds(UP_AT, RELAYED - UP_AT)]),
        (up.at[pl.ds(RELAYED - UP_AT, rest)], high.at[pl.ds(0, rest)]),
    ]
    for b in range(16):
        lanes = pl.ds(b * LANES, LANES)
        plan.append((down.at[:, lanes], high.at[pl.ds(rest + b * LANES, LANES)]))
    for i, part in enumerate((sgate, sup, sdown)):
        plan.append((part, shared_out.at[pl.ds(i * SHARED_UNITS, SHARED_UNITS)]))
        mine = part.at[pl.ds(core, HALF_UNITS)]
        plan.append((mine, half_out.at[pl.ds(i * HALF_UNITS, HALF_UNITS)]))
    copies = [pltpu.make_async_copy(s, d, sems.at[i]) for i, (s, d) in enumerate(plan)]
    for c in copies:
        c.start()
    for c in copies:
        c.wait()


def spread_body(shard, out, block, sems):
    move = pltpu.make_async_copy(shard, block, sems.at[16])
    move.start()
    move.wait()
    copies = [pltpu.make_async_copy(block, out.at[i], sems.at[i]) for i in range(16)]
    for c in copies:
        c.start()
    for c in copies:
        c.wait()


def mixer_body(
    at,
    docs,
    routes,
    scale,
    gain,
    bias,
    near,
    halo,
    weight,
    send,
    normed,
    own,
    weight_v,
    mixed_v,
    first_v,
    quarter_v,
    send_v,
    pick_v,
    sems,
):
    y, x = at[0], at[1]
    copies = [pltpu.make_async_copy(weight.at[g], weight_v.at[g], sems.at[g]) for g in range(4)]
    copies[0].start()
    own_row = (docs[...] + 1).astype(F32)
    own_marks = as_column(own_row)
    halo_row = halo[16].astype(F32).T[0:1]
    apart = iota((TOKENS_HERE, TOKENS_HERE), 0) - iota((TOKENS_HERE, TOKENS_HERE), 1)
    inside = (side([own_marks, own_marks]) == own_row) & (apart >= 0)
    corner = iota((HALO, HALO), 0) - iota((HALO, HALO), 1) + HALO
    corner_inside = own_marks[0:HALO, 0:HALO] == halo_row
    for g in range(4):
        window = 2 << g
        band = jnp.where(inside & (apart < window), 1.0, 0.0)
        edge = jnp.where(corner_inside & (corner < window), 1.0, 0.0)
        members = jnp.sum(band, axis=1, keepdims=True)
        first_members = members[0:HALO] + jnp.sum(edge, axis=1, keepdims=True)
        scale_by = 1.0 / jnp.concatenate([first_members, members[HALO:]], axis=0)
        band, edge = band.astype(BF16), edge.astype(BF16)
        for j in range(2):
            at_lane = slice(j * 2 * LANES, (j + 1) * 2 * LANES)
            mine = side([near[4 * g + 2 * j], near[4 * g + 2 * j + 1]])
            head = side([halo[4 * g + 2 * j], halo[4 * g + 2 * j + 1]])
            running = jnp.dot(band, mine, preferred_element_type=F32)
            begin = running[0:HALO] + jnp.dot(edge, head, preferred_element_type=F32)
            running = jnp.concatenate([begin, running[HALO:]], axis=0)
            mixed_v[g, :, at_lane] = (running * scale_by - mine.astype(F32)).astype(BF16)
        if g < 3:
            copies[g + 1].start()
    named = routes[...]
    dests = []
    for k, rank in enumerate(ranks_of(named)):
        slot = named[k : k + 1] * SLOTS_SENT + (rank >> 2)
        dests.append(jnp.where((rank & 3) == x, slot, -1))
    slot = iota((EXPERTS * SLOTS_SENT, TOKENS_HERE), 0)
    pick_v[...] = chosen((slot == dests[0]) | (slot == dests[1]))
    total = jnp.zeros((TOKENS_HERE, 1), F32)
    squares = jnp.zeros((TOKENS_HERE, 1), F32)
    for g in range(4):
        copies[g].wait()
        for j in range(2):
            at_lane = slice(j * 2 * LANES, (j + 1) * 2 * LANES)
            lanes = slice(g * QUARTER + j * 2 * LANES, g * QUARTER + (j + 1) * 2 * LANES)
            projected = jnp.dot(mixed_v[g], weight_v[g, :, at_lane], preferred_element_type=F32)
            mine = side([near[4 * g + 2 * j], near[4 * g + 2 * j + 1]]).astype(F32)
            first = RESIDUAL_SCALE * mine + projected * scale[:, lanes]
            first_v[g, :, at_lane] = first
            part, part_squares = sums(first)
            total = total + part
            squares = squares + part_squares
    mean = total / MODEL
    inv = lax.rsqrt(squares / MODEL - mean * mean + NORM_EPS)
    lanes = pl.ds(pl.multiple_of(y * QUARTER, QUARTER), QUARTER)
    gain_here, bias_here = gain[:, lanes], bias[:, lanes]
    for r in range(0, TOKENS_HERE, 64):
        rows = slice(r, r + 64)
        scaled = (first_v[y, rows, :] - mean[rows]) * inv[rows]
        quarter_v[rows, :] = (scaled * gain_here + bias_here).astype(BF16)
    quarter = quarter_v[...]
    send_v[...] = jnp.dot(pick_v[...], quarter, preferred_element_type=F32).astype(BF16)
    leave = pltpu.make_async_copy(send_v, send, sems.at[4])
    leave.start()
    mine = quarter[:, 0:LANES]
    for i in range(1, 4):
        mine = jnp.where(x == i, quarter[:, i * LANES : (i + 1) * LANES], mine)
    own[...] = mine
    upper = (y & 1) == 1
    half = pl.multiple_of((y & 1) * SHARED_ROWS, SHARED_ROWS)
    mean = jnp.where(upper, mean[SHARED_ROWS:], mean[:SHARED_ROWS])
    inv = jnp.where(upper, inv[SHARED_ROWS:], inv[:SHARED_ROWS])
    for r in range(0, SHARED_ROWS, 64):
        rows = slice(r, r + 64)
        for g in range(4):
            lanes = slice(g * QUARTER, (g + 1) * QUARTER)
            scaled = (first_v[g, pl.ds(half + r, 64), :] - mean[rows]) * inv[rows]
            normed[g, rows, :] = (scaled * gain[:, lanes] + bias[:, lanes]).astype(BF16)
    leave.wait()


def compact_body(rows, out):
    shape = (ROUTED_ROWS, EXPERTS * SLOTS_SENT)
    came = iota(shape, 1)
    within = came & 7
    goes = SLOTS_USED * (came >> 3) + within
    keep = chosen((iota(shape, 0) == goes) & (within < SLOTS_USED))
    packed = jnp.dot(keep, rows[...], preferred_element_type=F32).astype(BF16)
    for i in range(4):
        out[i] = packed


def shared_body(normed, s0, s1, s2, out, own_v, near_v, far_v, part_v, sems):
    copies = [
        pltpu.make_async_copy(source, target, sems.at[i])
        for i, (source, target) in enumerate(((s0, own_v), (s1, near_v), (s2, far_v)))
    ]
    for c in copies:
        c.start()
    shared = side([normed[i] for i in range(4)])
    for c in copies:
        c.wait()

    def units(i, lanes):
        here = slice(i * SHARED_UNITS, (i + 1) * SHARED_UNITS)
        half = slice(i * HALF_UNITS, (i + 1) * HALF_UNITS)
        return jnp.concatenate([own_v[here, lanes], near_v[half, lanes], far_v[half, lanes]], axis=0)

    contract = (((1,), (1,)), ((), ()))
    every = slice(0, MODEL)
    sg = lax.dot_general(shared, units(0, every), contract, preferred_element_type=F32)
    su = lax.dot_general(shared, units(1, every), contract, preferred_element_type=F32)
    hidden = (jax.nn.silu(sg) * su).astype(BF16)
    for b in range(0, 16, 2):
        down = units(2, slice(b * LANES, (b + 2) * LANES))
        part = jnp.dot(hidden, down, preferred_element_type=F32).astype(BF16)
        part_v[b] = part[:, :LANES]
        part_v[b + 1] = part[:, LANES:]
    send = pltpu.make_async_copy(part_v, out.at[:, pl.ds(ROUTED_ROWS, SHARED_ROWS), :], sems.at[3])
    send.start()
    send.wait()


def expert_body(rows, w0, w1, w2, w3, w4, w5, w6, w7, begun, out, wv, part_v, sems):
    moved = (w1, w2, w3, w4, w5, w6, w7)
    copies = [pltpu.make_async_copy(m, wv.at[i], sems.at[i]) for i, m in enumerate(moved)]
    for c in copies:
        c.start()
    shards = (w0,) + tuple(wv.at[i] for i in range(7))

    def lower(c, start, stop):
        return shards[2 * c][start:stop, :]

    def upper(c, start, stop):
        return shards[2 * c + 1][start - RELAYED : stop - RELAYED, :]

    tokens = side([rows[i] for i in range(4)])
    hidden = []
    for c in range(4):
        for i in ((0,), (1, 2), (3, 4), (5, 6))[c]:
            copies[i].wait()
        ups = [lower(c, UP_AT, RELAYED), upper(c, RELAYED, DOWN_AT)]
        both = side([lower(c, 0, UP_AT), jnp.concatenate(ups, axis=0)])
        parts = jnp.dot(tokens, both, preferred_element_type=F32)
        hidden.append((jax.nn.silu(parts[:, :LANES]) * parts[:, LANES:]).astype(BF16))
    hidden = side(hidden)

    def block(c, b):
        return upper(c, DOWN_AT + b * LANES, DOWN_AT + (b + 1) * LANES)

    sends = []
    for b in range(0, 16, 2):
        down = jnp.concatenate([side([block(c, b), block(c, b + 1)]) for c in range(4)], axis=0)
        part = jnp.dot(hidden, down, preferred_element_type=F32).astype(BF16)
        part_v[b] = part[:, :LANES]
        part_v[b + 1] = part[:, LANES:]
        target = out.at[pl.ds(b, 2), pl.ds(0, ROUTED_ROWS), :]
        sends.append(pltpu.make_async_copy(part_v.at[pl.ds(b, 2)], target, sems.at[7 + b // 2]))
        sends[-1].start()
    for c in sends:
        c.wait()


def return_body(parts, send, shared):
    routed = []
    for x in range(4):
        total = parts[x, 0:ROUTED_ROWS, :].astype(F32)
        for y in range(1, 4):
            total = total + parts[4 * y + x, 0:ROUTED_ROWS, :].astype(F32)
        routed.append(total.astype(BF16))
    for half in range(2):
        total = jnp.zeros((SHARED_ROWS, LANES), F32)
        for y in (half, half + 2):
            for x in range(4):
                total = total + parts[4 * y + x, ROUTED_ROWS:, :].astype(F32)
        shared[half * SHARED_ROWS : (half + 1) * SHARED_ROWS, :] = total
    rows = jnp.concatenate(routed, axis=0)
    count = 4 * ROUTED_ROWS
    came = iota((1, count), 1)
    x = (
        (came >= ROUTED_ROWS).astype(jnp.int32)
        + (came >= 2 * ROUTED_ROWS).astype(jnp.int32)
        + (came >= 3 * ROUTED_ROWS).astype(jnp.int32)
    )
    within = came - ROUTED_ROWS * x
    source = (within * 10923) >> 16
    goes = 18 * source + 6 * x + within
    move = chosen(iota((count, count), 0) == goes)
    send[...] = jnp.dot(move, rows, preferred_element_type=F32).astype(BF16)


def weigh_body(routes, weight, high_out, low_out):
    named = routes[...]
    scale = weight[...]
    slot = iota((4 * ROUTED_ROWS, TOKENS_HERE), 0)
    taken = jnp.zeros(slot.shape, F32)
    for k, rank in enumerate(ranks_of(named)):
        at = named[k : k + 1] * (4 * SLOTS_USED) + SLOTS_USED * (rank & 3) + (rank >> 2)
        taken = jnp.where(slot == at, scale[k : k + 1], taken)
    taken = taken.T
    high = taken.astype(BF16)
    high_out[...] = high
    low_out[...] = (taken - high.astype(F32)).astype(BF16)


def combine_body(rows, high, low, own, shared, second_out, stats_out):
    mix = jnp.dot(high[...], rows[...], preferred_element_type=F32)
    mix = mix + jnp.dot(low[...], rows[...], preferred_element_type=F32)
    second = RESIDUAL_SCALE * own[...].astype(F32) + mix + shared[...]
    second_out[...] = second
    stats = row_stats(second)[0:2]
    for i in range(16):
        stats_out[i] = stats


def settle_body(second, stats, gain, bias, out):
    total = stats[0]
    for i in range(1, 16):
        total = total + stats[i]
    mean, inv = mean_and_scale(total)
    out[...] = ((second[...] - mean) * inv * gain[...] + bias[...]).astype(BF16)


def struct(shape, dtype):
    return pltpu.HBM(shape, dtype)


def held(shape, dtype):
    return pltpu.VMEM(shape, dtype)


def exchange(parts, axes):
    return lax.all_to_all(parts, axes, split_axis=0, concat_axis=0, tiled=True)


def around(shard, by):
    return lax.ppermute(shard, "x", [(i, (i + by) % 4) for i in range(4)])


def kernel(body, in_specs, **options):
    params = pltpu.CompilerParams(vmem_limit_bytes=24 * 1024 * 1024)
    call = pl.pallas_call(body, in_specs=in_specs, compiler_params=params, **options)
    places = {id(HELD): pltpu.VMEM, id(HBM): pltpu.HBM}

    def run(*args):
        args = [
            pltpu.with_memory_space_constraint(a, places[id(s)]) if id(s) in places else a
            for a, s in zip(args, in_specs, strict=True)
        ]
        return call(*args)

    return run


def layer(
    layer_input,
    doc_ids,
    routes,
    route_weight,
    pool_weight,
    pool_scale,
    norm1_gain,
    norm1_bias,
    expert_gate,
    expert_up,
    expert_down,
    shared_gate,
    shared_up,
    shared_down,
    norm2_gain,
    norm2_bias,
):
    core = lax.axis_index("sp") & 1
    at = jnp.stack([lax.axis_index("y"), lax.axis_index("x"), core]).astype(jnp.int32)
    spread = kernel(
        spread_body,
        out_shape=struct((16, TOKENS_HERE, LANES), BF16),
        in_specs=[HBM],
        out_specs=HBM,
        scratch_shapes=[
            pltpu.VMEM((TOKENS_HERE, LANES), BF16),
            pltpu.SemaphoreType.DMA((17,)),
        ],
    )(layer_input)
    near = exchange(spread, ("y", "x"))
    low, high, shared_packed, shared_half = kernel(
        pack_body,
        out_shape=[
            held((RELAYED, LANES), BF16),
            held((RELAYED, LANES), BF16),
            struct((3 * SHARED_UNITS, MODEL), BF16),
            struct((3 * HALF_UNITS, MODEL), BF16),
        ],
        in_specs=[SMEM] + [HBM] * 6,
        out_specs=[VMEM] * 4,
        scratch_shapes=[pltpu.SemaphoreType.DMA((25,))],
        cost_estimate=pl.CostEstimate(
            flops=10_000_000, bytes_accessed=4 * PACKED * LANES, transcendentals=0
        ),
    )(
        at,
        expert_gate[0],
        expert_up[0],
        expert_down[0],
        shared_gate.T,
        shared_up.T,
        shared_down,
    )
    marks = jnp.broadcast_to((doc_ids[-HALO:] + 1).astype(BF16)[:, None], (HALO, LANES))
    tail = jnp.concatenate([near[:, -HALO:, :], marks[None]], axis=0)
    following = [(i, i + 1) for i in range(lax.axis_size("sp") - 1)]
    halo = lax.ppermute(tail, "sp", following)
    left_low = around(low, 1)
    right_high = around(high, -1)
    left_high = around(high, 1)
    right_low = around(low, -1)
    send, normed, own = kernel(
        mixer_body,
        in_specs=[SMEM] + [VMEM] * 5 + [HELD, HELD, HBM],
        out_specs=[HBM, VMEM, VMEM],
        scratch_shapes=[
            pltpu.VMEM((4, QUARTER, QUARTER), BF16),
            pltpu.VMEM((4, TOKENS_HERE, QUARTER), BF16),
            pltpu.VMEM((4, TOKENS_HERE, QUARTER), F32),
            pltpu.VMEM((TOKENS_HERE, QUARTER), BF16),
            pltpu.VMEM((EXPERTS * SLOTS_SENT, QUARTER), BF16),
            pltpu.VMEM((EXPERTS * SLOTS_SENT, TOKENS_HERE), BF16),
            pltpu.SemaphoreType.DMA((5,)),
        ],
        out_shape=[
            struct((EXPERTS * SLOTS_SENT, QUARTER), BF16),
            held((4, SHARED_ROWS, QUARTER), BF16),
            held((TOKENS_HERE, LANES), BF16),
        ],
    )(
        at,
        doc_ids[None],
        routes.T,
        pool_scale[None],
        norm1_gain[None],
        norm1_bias[None],
        near,
        halo,
        pool_weight,
    )
    from_pair = lax.ppermute(shared_half, "y", [(i, i ^ 1) for i in range(4)])
    cores = [(i, i ^ 1) for i in range(lax.axis_size("sp"))]
    from_core = lax.ppermute(from_pair, "sp", cores)
    across_low = around(left_low, 1)
    across_high = around(right_high, -1)
    arrived = exchange(send.reshape(EXPERTS, SLOTS_SENT, QUARTER), "sp")
    gather_in = kernel(
        compact_body,
        out_shape=struct((4, ROUTED_ROWS, QUARTER), BF16),
        in_specs=[HELD],
        out_specs=VMEM,
    )(arrived.reshape(EXPERTS * SLOTS_SENT, QUARTER))
    gathered = exchange(gather_in, "y")
    begun = kernel(
        shared_body,
        out_shape=struct((16, ROUTED_ROWS + SHARED_ROWS, LANES), BF16),
        in_specs=[HELD, HBM, HBM, ANY],
        out_specs=HBM,
        scratch_shapes=[
            pltpu.VMEM((3 * SHARED_UNITS, MODEL), BF16),
            pltpu.VMEM((3 * HALF_UNITS, MODEL), BF16),
            pltpu.VMEM((3 * HALF_UNITS, MODEL), BF16),
            pltpu.VMEM((16, SHARED_ROWS, LANES), BF16),
            pltpu.SemaphoreType.DMA((4,)),
        ],
    )(normed, shared_packed, from_pair, from_core)
    partial = kernel(
        expert_body,
        out_shape=struct((16, ROUTED_ROWS + SHARED_ROWS, LANES), BF16),
        in_specs=[HELD] * 2 + [HBM] * 8,
        out_specs=HBM,
        scratch_shapes=[
            pltpu.VMEM((7, RELAYED, LANES), BF16),
            pltpu.VMEM((16, ROUTED_ROWS, LANES), BF16),
            pltpu.SemaphoreType.DMA((15,)),
        ],
        input_output_aliases={9: 0},
    )(
        gathered,
        low,
        high,
        left_low,
        left_high,
        right_low,
        right_high,
        across_low,
        across_high,
        begun,
    )
    parts = exchange(partial, ("y", "x"))
    back, shared_sum = kernel(
        return_body,
        out_shape=[
            struct((4 * ROUTED_ROWS, LANES), BF16),
            held((TOKENS_HERE, LANES), F32),
        ],
        in_specs=[HELD],
        out_specs=[VMEM, VMEM],
    )(parts)
    returned = exchange(back.reshape(EXPERTS, 4 * SLOTS_USED, LANES), "sp")
    high_weights, low_weights = kernel(
        weigh_body,
        out_shape=[held((TOKENS_HERE, 4 * ROUTED_ROWS), BF16)] * 2,
        in_specs=[VMEM] * 2,
        out_specs=[VMEM] * 2,
    )(routes.T, route_weight.T)
    second, row_sums = kernel(
        combine_body,
        out_shape=[held((TOKENS_HERE, LANES), F32), struct((16, 2, TOKENS_HERE), F32)],
        in_specs=[HELD] * 5,
        out_specs=[VMEM, VMEM],
    )(returned.reshape(4 * ROUTED_ROWS, LANES), high_weights, low_weights, own, shared_sum)
    row_sums = exchange(row_sums, ("y", "x"))
    return kernel(
        settle_body,
        out_shape=jax.ShapeDtypeStruct((TOKENS_HERE, LANES), BF16),
        in_specs=[HELD, HELD, VMEM, VMEM],
        out_specs=VMEM,
    )(second, row_sums, norm2_gain[None], norm2_bias[None])


def solution(mesh):
    split = Mesh(mesh.devices.reshape(mesh.shape["sp"], 4, 4), ("sp", "y", "x"))
    tp = ("y", "x")
    placed = (
        P("sp", tp),
        P("sp"),
        P("sp", None),
        P("sp", None),
        P(),
        P(),
        P(),
        P(),
        P("sp", None, tp),
        P("sp", None, tp),
        P("sp", tp, None),
        P(None, tp),
        P(None, tp),
        P(tp, None),
        P(tp),
        P(tp),
    )
    return jax.shard_map(layer, mesh=split, in_specs=placed, out_specs=P("sp", tp), check_vma=False)
```
